256 devices in a mesh: ep: 64 (over z, x, core), tp: 4 (over y).
Axes of the slice: x: 4, y: 4, z: 8, core: 2. Of those that a mesh axis runs over, the one named last changes fastest.
Arguments:
- tokens: bfloat16 [1024, 2048], P('ep'), may hold values from -6 to 6
- attn_gain: float32 [2048], replicated, may hold values from 0.1 to 1.9
- query_weight: bfloat16 [2048, 2048], P('ep', 'tp'), may hold values from -0.125 to 0.125
- key_weight: bfloat16 [2048, 512], P('ep', 'tp'), may hold values from -0.125 to 0.125
- value_weight: bfloat16 [2048, 512], P('ep', 'tp'), may hold values from -0.125 to 0.125
- break_bias: float32 [16], P('tp'), may hold values from -14 to -8
- cache_keys: bfloat16 [1024, 4, 1024, 128], P('ep', 'tp'), may hold values from -18 to 18
- cache_values: bfloat16 [1024, 4, 1024, 128], P('ep', 'tp'), may hold values from -6 to 6
- lengths: int32 [1024], P('ep'), may hold values from 1 to 1024, 524288 in all
- out_weight: bfloat16 [2048, 2048], P('tp', 'ep'), may hold values from -0.25 to 0.25
- ffn_gain: float32 [2048], replicated, may hold values from 0.1 to 1.9
- branch_gate: bfloat16 [2048], replicated, may hold values from -0.125 to 0.125
- dense_gate: bfloat16 [2048, 8192], P('tp', 'ep'), may hold values from -0.125 to 0.125
- dense_up: bfloat16 [2048, 8192], P('tp', 'ep'), may hold values from -0.125 to 0.125
- dense_down: bfloat16 [8192, 2048], P('ep', 'tp'), may hold values from -0.0625 to 0.0625
- route_ids: int32 [1024, 4], P('ep'), may hold values from 0 to 63, all different within a row; in each aligned block of 16 rows (0 to 15, 16 to 31, ...) at most 2 rows name the same one
- route_weights: float32 [1024, 4], P('ep'), may hold values from 0.1 to 1
- expert_gate: bfloat16 [64, 2048, 1024], P('ep', None, 'tp'), may hold values from -0.4375 to 0.4375
- expert_up: bfloat16 [64, 2048, 1024], P('ep', None, 'tp'), may hold values from -0.4375 to 0.4375
- expert_down: bfloat16 [64, 1024, 2048], P('ep', 'tp'), may hold values from -0.01953125 to 0.01953125
Outputs:
- layer_out: bfloat16 [1024, 2048], P('ep', 'tp')
- new_keys: bfloat16 [1024, 512], P('ep', 'tp')
- new_values: bfloat16 [1024, 512], P('ep', 'tp')
The draws below stay inside these ranges and needn't reach their ends.
Inputs may be any that keep to these rules, and one draw needn't show every extreme that they name: `route_ids`: each row names 4 different experts. Among the rows of one device no expert is named more than 2 times, a bound that some block reaches. Sequence b's cache holds keys at positions below lengths[b]; some sequence fills its whole cache.
All inputs are finite; a program needn't handle non-finite values. No bound on the sum of `lengths` on one device may be relied on, other than what follows from the above.
Results may differ from the reference program's by a relative error of at most 0.011.
Values may be sent and summed in bfloat16 or wider, within the bound.
No kernel may reach another device: no remote copies, remote signals or barrier semaphores. Data moves between devices by JAX's collectives and lax.ppermute only.
A program may use at most 64 MiB of HBM per device.

```python
import math
import jax
import jax.numpy as jnp
import numpy as np
from jax import lax

D = 2048
HEADS = 16
KV_HEADS = 4
HEAD_DIM = 128
DENSE = 8192
EXPERT_W = 1024
TOP_K = 4
SEQS = 16
CACHE_LEN = 1024
SEQUENCES = 1024
EXPERTS = 64
CAP = 2
N_EP = 64


def levels(key, extent, split, smallest, high):
    def one(axis_at, shards_of):
        draws = jax.random.uniform(jax.random.fold_in(jax.random.fold_in(key, 6), axis_at), (shards_of,), jnp.float32, smallest / len(split), high / len(split))
        return jnp.repeat(jnp.exp(draws), extent[axis_at] // shards_of).reshape((-1,) + (1,) * (len(extent) - axis_at - 1))

    loudness = one(*split[0])
    for cut in split[1:]:
        loudness = loudness * one(*cut)
    return loudness


def split_up(count, total, most, slope):
    loads = [(1 << 20) // math.isqrt(standing ** slope) + 1 for standing in range(2, count + 1)]
    spare, counts = total - most - (count - 1), [1] * (count - 1)
    while spare > 0:
        candidates = [i for i in range(count - 1) if counts[i] < most]
        pool, budget = sum([loads[i] for i in candidates]), spare
        for i in candidates:
            extra = min(most - counts[i], max(1, budget * loads[i] // pool), spare)
            counts[i] = counts[i] + extra
            spare = spare - extra
    return np.array([most] + counts)


def uneven_parts(rng, amount, total, reach, slope):
    if amount == 2:
        one = jax.random.randint(rng, (), max(1, total - reach), min(reach, total - 1) + 1)
        return jnp.stack([one, total - one])
    tallies = jnp.asarray(split_up(amount, total, reach, slope), jnp.int32)
    twos = (amount - 1) // 2
    giver, taker = tallies[1:1 + 2 * twos:2], tallies[2:2 + 2 * twos:2]
    slack = jnp.minimum(giver - 1, reach - taker)
    moved = jax.random.randint(jax.random.fold_in(rng, 1), (twos,), 0, 1 << 20) % (slack + 1)
    tallies = tallies.at[1:1 + 2 * twos:2].set(giver - moved).at[2:2 + 2 * twos:2].set(taker + moved)
    return tallies[jax.random.permutation(jax.random.fold_in(rng, 2), amount)]


def assign_block(key, own, number, rows, amount, top, most, lean):
    order = jax.random.permutation(key, amount)
    heavy_load, usual = portions_of(amount, rows * top, most, lean, True), portions_of(amount, rows * top, most, lean, False)
    places = jnp.arange(amount)

    def named(sizes, rotation):
        used = int((sizes > 0).sum())
        fixed = max(1, used // 4)
        moved = fixed + (places - fixed + rotation * (used - fixed)) % max(1, amount - fixed)
        return jnp.zeros((amount,), jnp.int32).at[order[jnp.where(places < fixed, places, moved)]].set(jnp.asarray(sizes, jnp.int32))

    sizes = jnp.where(number % 4 == 0, named(heavy_load, number // 4), named(usual, number - number // 4 - 1))
    mixed = jax.random.permutation(jax.random.fold_in(own, 3), amount)
    donor, taker = mixed[0:amount // 2 * 2:2], mixed[1:amount // 2 * 2:2]
    room = jnp.minimum(sizes[donor] - 1, most - sizes[taker]) // 2
    room = jnp.where((donor == order[0]) | (taker == order[0]) | (sizes[taker] == 0), 0, jnp.maximum(room, 0))
    moved = jax.random.randint(jax.random.fold_in(own, 4), (amount // 2,), 0, 1 << 20) % (room + 1)
    sizes = sizes.at[donor].add(-moved).at[taker].add(moved)
    labels = jnp.searchsorted(jnp.cumsum(sizes), jnp.arange(rows * top), side="right").astype(jnp.int32)
    grid = labels.reshape(top, rows).T
    grid = grid[jax.random.permutation(jax.random.fold_in(own, 1), rows)]
    rotation = jax.random.randint(jax.random.fold_in(own, 2), (rows, 1), 0, top)
    return jnp.take_along_axis(grid, (jnp.arange(top)[None, :] + rotation) % top, axis=1)


def portions_of(number_of, total, limit, slope, full):
    weights = [(1 << 20) // math.isqrt(standing ** slope) + 1 for standing in range(1, number_of + 1)]
    largest = limit if full else min(limit, max(-(-total // number_of), total * weights[0] // sum(weights)))
    least = 1 if total - largest >= number_of - 1 else 0
    holding, spare = [largest] + [least] * (number_of - 1), total - largest - least * (number_of - 1)
    while spare > 0:
        candidates = [i for i in range(1, number_of) if holding[i] < largest] or [i for i in range(1, number_of) if holding[i] < limit]
        pool, budget = sum([weights[i] for i in candidates]), spare
        for i in candidates:
            addition = min(limit - holding[i], max(1, budget * weights[i] // pool), spare)
            holding[i] = holding[i] + addition
            spare = spare - addition
    return np.array(holding)


def normal_values(rng, shape, width, limit, pieces=(), held_as=jnp.bfloat16):
    entries = width * jax.random.normal(rng, shape, jnp.float32)
    if pieces:
        entries = entries * levels(rng, shape, pieces, -0.22, 0.18)
    return jnp.clip(entries, -limit, limit).astype(held_as)


def setup_inputs(seed: int = 0) -> dict:
    splits = jax.random.split(jax.random.key(seed), 21)
    tokens = normal_values(splits[0], (SEQUENCES, D), 1.0, 6.0, ((0, 64),))
    attn_gain = jnp.clip(1.0 + 0.18 * jax.random.normal(splits[1], (D,), jnp.float32), 0.1, 1.9)
    query_weight = normal_values(splits[2], (D, HEADS * HEAD_DIM), D ** -0.5, 0.125, ((0, 64), (1, 4)))
    key_weight = normal_values(splits[3], (D, KV_HEADS * HEAD_DIM), D ** -0.5, 0.125, ((0, 64), (1, 4)))
    value_weight = normal_values(splits[4], (D, KV_HEADS * HEAD_DIM), D ** -0.5, 0.125, ((0, 64), (1, 4)))
    break_bias = jnp.clip(-14.0 + 6.0 * jax.random.uniform(splits[5], (HEADS,), jnp.float32) ** levels(splits[5], (HEADS,), ((0, 4),), -0.2, 0.2), -14.0, -8.0)
    cache_keys = normal_values(splits[6], (SEQUENCES, KV_HEADS, CACHE_LEN, HEAD_DIM), 3.0, 18.0, ((0, 64), (1, 4)))
    cache_values = normal_values(splits[7], (SEQUENCES, KV_HEADS, CACHE_LEN, HEAD_DIM), 1.0, 6.0, ((0, 64), (1, 4)))
    lengths = uneven_parts(splits[8], SEQUENCES, SEQUENCES * CACHE_LEN // 2, CACHE_LEN, 2).astype(jnp.int32)
    out_weight = normal_values(splits[9], (HEADS * HEAD_DIM, D), (HEADS * HEAD_DIM // 4) ** -0.5, 0.25, ((0, 4), (1, 64)))
    ffn_gain = jnp.clip(1.0 + 0.18 * jax.random.normal(splits[10], (D,), jnp.float32), 0.1, 1.9)
    branch_gate = normal_values(splits[11], (D,), D ** -0.5, 0.125)
    dense_gate = normal_values(splits[12], (D, DENSE), D ** -0.5, 0.125, ((0, 4), (1, 64)))
    dense_up = normal_values(splits[13], (D, DENSE), D ** -0.5, 0.125, ((0, 4), (1, 64)))
    dense_down = normal_values(splits[14], (DENSE, D), DENSE ** -0.5, 0.0625, ((0, 64), (1, 4)))
    route_ids_keys = jax.random.split(jax.random.fold_in(splits[15], 1), SEQUENCES // SEQS)
    route_ids_turns = jax.random.permutation(jax.random.fold_in(splits[15], 3), SEQUENCES // SEQS)
    route_ids = jax.vmap(lambda own, number: assign_block(jax.random.fold_in(splits[15], 2), own, number, SEQS, EXPERTS, TOP_K, CAP, 2))(route_ids_keys, route_ids_turns).reshape((SEQUENCES, TOP_K))
    route_weights = jnp.clip(jnp.exp(math.log(1.0) - 2.3025851 * jax.random.uniform(splits[16], (SEQUENCES, TOP_K), jnp.float32) ** levels(splits[16], (SEQUENCES, TOP_K), ((0, 64),), -0.2, 0.2)), 0.1, 1.0)
    expert_gate = normal_values(splits[17], (EXPERTS, D, EXPERT_W), (D // 12) ** -0.5, 0.4375, ((0, 64), (2, 4)))
    expert_up = normal_values(splits[18], (EXPERTS, D, EXPERT_W), (D // 12) ** -0.5, 0.4375, ((0, 64), (2, 4)))
    expert_down = normal_values(splits[19], (EXPERTS, EXPERT_W, D), (EXPERT_W * 80) ** -0.5, 0.01953125, ((0, 64), (1, 4)))
    return {"tokens": tokens, "attn_gain": attn_gain, "query_weight": query_weight, "key_weight": key_weight, "value_weight": value_weight, "break_bias": break_bias, "cache_keys": cache_keys, "cache_values": cache_values, "lengths": lengths, "out_weight": out_weight, "ffn_gain": ffn_gain, "branch_gate": branch_gate, "dense_gate": dense_gate, "dense_up": dense_up, "dense_down": dense_down, "route_ids": route_ids, "route_weights": route_weights, "expert_gate": expert_gate, "expert_up": expert_up, "expert_down": expert_down}


norm_eps = 1e-05
clamp_limit = 7.0
swish_alpha = 1.702

def rms_scale(values, gain):
    return values * lax.rsqrt(lax.optimization_barrier(jnp.mean(values * values, axis=-1, keepdims=True)) + norm_eps) * gain

def clamped_unit(gate_pre, up_pre):
    gate_c = jnp.minimum(gate_pre, clamp_limit)
    up_c = jnp.clip(up_pre, -clamp_limit, clamp_limit)
    return (up_c + 1.0) * gate_c * jax.nn.sigmoid(swish_alpha * gate_c)

def reference(tokens, attn_gain, query_weight, key_weight, value_weight, break_bias, cache_keys, cache_values, lengths, out_weight, ffn_gain, branch_gate, dense_gate, dense_up, dense_down, route_ids, route_weights, expert_gate, expert_up, expert_down):
    normed = rms_scale(tokens.astype(jnp.float32), attn_gain).astype(jnp.bfloat16)
    queries = jnp.dot(normed, query_weight, preferred_element_type=jnp.float32).astype(jnp.bfloat16)
    new_keys = jnp.dot(normed, key_weight, preferred_element_type=jnp.float32).astype(jnp.bfloat16)
    new_values = jnp.dot(normed, value_weight, preferred_element_type=jnp.float32).astype(jnp.bfloat16)
    group_size = HEADS // KV_HEADS
    query_heads = queries.reshape(SEQUENCES, KV_HEADS, group_size, HEAD_DIM)
    head_bias = break_bias.reshape(KV_HEADS, group_size)
    positions = jnp.arange(CACHE_LEN, dtype=jnp.int32)

    def one_sequence(packed):
        query_rows, key_rows, value_rows, length_now = packed
        scores = jnp.einsum('grd,gld->grl', query_rows.astype(jnp.float32), key_rows.astype(jnp.float32))
        scores = scores * HEAD_DIM ** (-0.5) + head_bias[:, :, None]
        inside = (positions < length_now)[None, None, :]
        log_keep = jnp.where(inside, jax.nn.log_sigmoid(-scores), 0.0)
        between = lax.cumsum(log_keep, axis=2, reverse=True) - log_keep
        weights = jnp.where(inside, jnp.exp(jax.nn.log_sigmoid(scores) + between), 0.0).astype(jnp.bfloat16)
        return jnp.einsum('grl,gld->grd', weights.astype(jnp.float32), value_rows.astype(jnp.float32)).astype(jnp.bfloat16)
    attended = lax.map(one_sequence, (query_heads, cache_keys, cache_values, lengths))
    attended = attended.reshape(SEQUENCES, HEADS * HEAD_DIM)
    mixed = jnp.dot(attended, out_weight, preferred_element_type=jnp.float32).astype(jnp.bfloat16)
    resid = tokens.astype(jnp.float32) + mixed.astype(jnp.float32)
    normed2 = rms_scale(resid, ffn_gain).astype(jnp.bfloat16)
    slot_count = N_EP * CAP
    token_ids = jnp.arange(SEQUENCES, dtype=jnp.int32)

    def per_expert(expert_sum, expert):
        route_hits = route_ids == expert
        chosen = jnp.any(route_hits, axis=1)
        scale_sum = lax.optimization_barrier(jnp.sum(jnp.where(route_hits, route_weights, 0.0), axis=1))
        place_index = jnp.cumsum(chosen.astype(jnp.int32)) - 1
        target = jnp.where(chosen, place_index, slot_count).astype(jnp.int32)
        row_index = jnp.zeros((slot_count + 1,), jnp.int32).at[target].set(token_ids)[:slot_count]
        picked_rows = normed2[row_index]
        gate_pre = jnp.dot(picked_rows, expert_gate[expert], preferred_element_type=jnp.float32)
        up_pre = jnp.dot(picked_rows, expert_up[expert], preferred_element_type=jnp.float32)
        activation = clamped_unit(gate_pre, up_pre).astype(jnp.bfloat16)
        expert_rows = jnp.dot(activation, expert_down[expert], preferred_element_type=jnp.float32).astype(jnp.bfloat16)
        slot_live = jnp.arange(slot_count, dtype=jnp.int32) < jnp.sum(chosen.astype(jnp.int32))
        row_scale = jnp.where(slot_live, scale_sum[row_index], 0.0)
        return (expert_sum.at[row_index].add(row_scale[:, None] * expert_rows.astype(jnp.float32)), None)
    expert_sum, unused_out = lax.scan(per_expert, jnp.zeros((SEQUENCES, D), jnp.float32), jnp.arange(EXPERTS, dtype=jnp.int32))
    gate_part = jnp.dot(normed2, dense_gate, preferred_element_type=jnp.float32)
    up_part = jnp.dot(normed2, dense_up, preferred_element_type=jnp.float32)
    hidden_units = (jax.nn.silu(gate_part) * up_part).astype(jnp.bfloat16)
    dense_out = jnp.dot(hidden_units, dense_down, preferred_element_type=jnp.float32)
    branch_scale = jax.nn.sigmoid(jnp.dot(normed2, branch_gate, preferred_element_type=jnp.float32))
    layer_out = (resid + expert_sum + branch_scale[:, None] * dense_out).astype(jnp.bfloat16)
    return (layer_out, new_keys, new_values)
```

```python
import functools
import jax
import jax.numpy as jnp
from jax import lax
from jax.experimental import pallas as pl
from jax.experimental.pallas import tpu as pltpu
from jax.sharding import Mesh
from jax.sharding import PartitionSpec as P

EP = ("z", "x", "c")
ZX = ("z", "x")

norm_eps = 1e-05
clamp_limit = 7.0
swish_alpha = 1.702
f32 = jnp.float32
bf16 = jnp.bfloat16


def rms_scale(values, gain):
    return values * lax.rsqrt(jnp.mean(values * values, axis=-1, keepdims=True) + norm_eps) * gain


def clamped_unit(gate_pre, up_pre):
    gate_c = jnp.minimum(gate_pre, clamp_limit)
    up_c = jnp.clip(up_pre, -clamp_limit, clamp_limit)
    return (up_c + 1.0) * gate_c * jax.nn.sigmoid(swish_alpha * gate_c)


def exchange(blocks, axes):
    return lax.all_to_all(blocks, axes, 0, 0, tiled=True)


def to_everyone(shard, axes):
    count = lax.axis_size(axes)
    return exchange(jnp.broadcast_to(shard[None], (count, *shard.shape)), axes)


def other_core(values):
    return lax.ppermute(values, "c", [(0, 1), (1, 0)])


def attention_kernel(per_step, group, span, lengths_ref, q_ref, bias_ref, k_ref, v_ref, o_ref):
    step = pl.program_id(0)
    head_dim = k_ref.shape[-1]
    scores = []
    for i in range(per_step):
        q = q_ref[i]
        scores.append(
            lax.dot_general(
                q, k_ref[i, 0], (((1,), (1,)), ((), ())), preferred_element_type=f32
            )
        )
    z = jnp.concatenate(scores, axis=0) * head_dim ** (-0.5) + bias_ref[:, 0:1]
    rows = z.shape[0]
    row_group = lax.broadcasted_iota(jnp.int32, (rows, 1), 0) // group
    length = jnp.zeros((rows, 1), jnp.int32)
    for i in range(per_step):
        length = jnp.where(row_group == i, lengths_ref[step * per_step + i], length)
    inside = lax.broadcasted_iota(jnp.int32, (rows, span), 1) < length
    tail = jnp.log1p(jnp.exp(-jnp.abs(z)))
    keep = jnp.where(inside, -jnp.maximum(z, 0.0) - tail, 0.0)
    take = jnp.minimum(z, 0.0) - tail
    lane = lax.broadcasted_iota(jnp.int32, (rows, 128), 1)
    chunks = span // 128
    after = jnp.zeros((rows, 1), f32)
    betweens = [None] * chunks
    for c in range(chunks - 1, -1, -1):
        own = keep[:, c * 128 : (c + 1) * 128]
        total = own
        shift = 1
        while shift < 128:
            moved = pltpu.roll(total, 128 - shift, 1)
            total = total + jnp.where(lane < 128 - shift, moved, 0.0)
            shift *= 2
        betweens[c] = total - own + after
        after = after + total[:, 0:1]
    between = jnp.concatenate(betweens, axis=1)
    weights = jnp.where(inside, jnp.exp(take + between), 0.0).astype(bf16)
    for i in range(per_step):
        o_ref[i] = jnp.dot(
            weights[i * group : (i + 1) * group], v_ref[i, 0], preferred_element_type=f32
        ).astype(bf16)


def attention(queries, bias, keys, values, lengths):
    seqs, _, span, head_dim = keys.shape
    heads = queries.shape[1] // head_dim
    group = 8
    per_step = 4
    q = queries.reshape(seqs, heads, head_dim)
    q = jnp.pad(q, ((0, 0), (0, group - heads), (0, 0)))
    b = jnp.pad(bias, (0, group - heads))
    b = jnp.broadcast_to(jnp.tile(b, per_step)[:, None], (per_step * group, 128))
    out = pl.pallas_call(
        functools.partial(attention_kernel, per_step, group, span),
        grid_spec=pltpu.PrefetchScalarGridSpec(
            num_scalar_prefetch=1,
            grid=(seqs // per_step,),
            in_specs=[
                pl.BlockSpec((per_step, group, head_dim), lambda i, n: (i, 0, 0)),
                pl.BlockSpec((per_step * group, 128), lambda i, n: (0, 0)),
                pl.BlockSpec((per_step, 1, span, head_dim), lambda i, n: (i, 0, 0, 0)),
                pl.BlockSpec((per_step, 1, span, head_dim), lambda i, n: (i, 0, 0, 0)),
            ],
            out_specs=pl.BlockSpec((per_step, group, head_dim), lambda i, n: (i, 0, 0)),
        ),
        out_shape=jax.ShapeDtypeStruct((seqs, group, head_dim), bf16),
        name="attention",
    )(lengths, q, b, keys, values)
    return out[:, :heads].reshape(seqs, heads * head_dim)


def body(
    tokens,
    attn_gain,
    query_weight,
    key_weight,
    value_weight,
    break_bias,
    cache_keys,
    cache_values,
    lengths,
    out_weight,
    ffn_gain,
    branch_gate,
    dense_gate,
    dense_up,
    dense_down,
    route_ids,
    route_weights,
    expert_gate,
    expert_up,
    expert_down,
):
    nz, nx, nt = lax.axis_size("z"), lax.axis_size("x"), lax.axis_size("tp")
    nzx = nz * nx
    seqs, width = tokens.shape
    experts = nzx * 2
    cap = 2
    slice_width = width // nt
    tp_start = lax.axis_index("tp") * slice_width
    q_cols, k_cols = query_weight.shape[1], key_weight.shape[1]

    w_own = jnp.concatenate([query_weight, key_weight, value_weight], axis=1)
    normed = rms_scale(tokens.astype(f32), attn_gain).astype(bf16)
    w_part = to_everyone(w_own, ("x", "c")).reshape(-1, w_own.shape[1])
    feats = jnp.moveaxis(normed.reshape(seqs, nz, width // nz), 1, 0)
    feats = exchange(feats, "z").reshape(nz * seqs, width // nz)

    ow = to_everyone(out_weight.T, "z")
    ow = to_everyone(ow.reshape(-1, ow.shape[2]), "x")
    ow = ow.reshape(nx, nz, -1, ow.shape[2])
    ow_other = other_core(ow)

    eid = jnp.arange(experts, dtype=jnp.int32)
    hit = route_ids[:, :, None] == eid
    chosen = jnp.any(hit, axis=1)
    weight = jnp.sum(jnp.where(hit, route_weights[:, :, None], 0.0), axis=1)
    count = chosen.astype(jnp.int32)
    rank = jnp.cumsum(count, axis=0) - count
    row = jnp.arange(seqs, dtype=f32)[:, None]
    meta = []
    for s in range(cap):
        here = chosen & (rank == s)
        meta.append(jnp.sum(jnp.where(here, row, 0.0), axis=0))
        meta.append(jnp.sum(jnp.where(here, weight, 0.0), axis=0))
    meta = jnp.stack(meta, axis=1)
    meta = jnp.pad(meta, ((0, 0), (0, 128 - 2 * cap)))[:, None, :]
    meta = exchange(meta, EP)[:, 0, : 2 * cap].reshape(nzx, 2, cap, 2)
    core = lax.axis_index("c")
    meta = jnp.where(core == 0, meta, meta[:, ::-1])
    meta = jnp.moveaxis(meta, 1, 0)
    slot_rows = meta[..., 0].astype(jnp.int32)
    block_at = jnp.arange(2 * nzx, dtype=jnp.int32).reshape(2, nzx, 1) * seqs
    slot_rows = (slot_rows + block_at).reshape(-1)
    slot_weights = meta[..., 1].reshape(-1)
    slot_count = 2 * nzx * cap
    all_rows = 2 * nzx * seqs
    onehot = (slot_rows[:, None] == jnp.arange(all_rows, dtype=jnp.int32)[None, :]).astype(bf16)

    partial = jnp.dot(feats, w_part, preferred_element_type=f32).astype(bf16)
    partial = exchange(partial.reshape(nz, seqs, -1), "z")
    qkv = jnp.sum(partial.astype(f32), axis=0).astype(bf16)
    queries = qkv[:, :q_cols]
    new_keys = qkv[:, q_cols : q_cols + k_cols]
    new_values = qkv[:, q_cols + k_cols :]

    attended = attention(queries, break_bias, cache_keys, cache_values, lengths)

    both = jnp.stack(
        [jnp.where(core == 0, ow, ow_other), jnp.where(core == 0, ow_other, ow)], axis=2
    )
    both = jnp.moveaxis(both, 0, 1).reshape(width, -1)
    partial_out = lax.dot_general(
        attended, both, (((1,), (1,)), ((), ())), preferred_element_type=f32
    )
    mixed = to_everyone(partial_out.astype(bf16), "tp").astype(f32).sum(axis=0).astype(bf16)
    resid = tokens.astype(f32) + mixed.astype(f32)
    normed2 = rms_scale(resid, ffn_gain).astype(bf16)

    own_slice = lax.dynamic_slice_in_dim(normed2, tp_start, slice_width, 1)
    mine = to_everyone(own_slice, ZX)
    other = other_core(mine)
    rows_x = jnp.concatenate([mine, other], axis=0).reshape(all_rows, slice_width)

    gate_slice = lax.dynamic_slice_in_dim(branch_gate, tp_start, slice_width, 0)
    gu = jnp.concatenate([dense_gate, dense_up], axis=1)
    dense_pre = jnp.dot(rows_x, gu, preferred_element_type=f32).astype(bf16)
    branch_pre = jnp.dot(rows_x, gate_slice, preferred_element_type=f32)
    slot_x = jnp.dot(onehot, rows_x, preferred_element_type=f32).astype(bf16)
    quarter = all_rows // nt
    half = slice_width // 2
    slot_fold = jnp.concatenate([slot_x[:, :half], slot_x[:, half:]], axis=0)
    m1 = jnp.concatenate(
        [
            dense_pre.reshape(nt, quarter, 2 * dense_gate.shape[1]),
            jnp.broadcast_to(slot_fold[None], (nt, *slot_fold.shape)),
        ],
        axis=2,
    )
    tailrow = jnp.pad(
        branch_pre.astype(bf16).reshape(nt, 1, quarter), ((0, 0), (0, 15), (0, half * 2 - quarter))
    )
    m1 = exchange(jnp.concatenate([m1, tailrow], axis=1), "tp")
    pre = m1[:, :quarter, :half].astype(f32).sum(axis=0)
    cols = dense_gate.shape[1]
    branch = jax.nn.sigmoid(m1[:, quarter, :quarter].astype(f32).sum(axis=0))
    hidden = (jax.nn.silu(pre[:, :cols]) * pre[:, cols:] * branch[:, None]).astype(bf16)
    sx = m1[:, :quarter, half:]
    sx = jnp.concatenate([sx[:, :slot_count], sx[:, slot_count:]], axis=2)
    sx = jnp.moveaxis(sx, 0, 1).reshape(slot_count, width)
    gate_pre = jnp.dot(sx, expert_gate[0], preferred_element_type=f32)
    up_pre = jnp.dot(sx, expert_up[0], preferred_element_type=f32)
    act = clamped_unit(gate_pre, up_pre).astype(bf16)
    out_rows = jnp.dot(act, expert_down[0], preferred_element_type=f32).astype(bf16)
    out_rows = jnp.moveaxis(out_rows.reshape(slot_count, nt, slice_width), 1, 0)
    hid_fold = jnp.concatenate([hidden[:slot_count], hidden[slot_count:]], axis=1)
    m2 = jnp.concatenate(
        [out_rows, jnp.broadcast_to(hid_fold[None], (nt, *hid_fold.shape))], axis=2
    )
    m2 = exchange(m2, "tp")
    moe_rows = m2[:, :, :slice_width].astype(f32).sum(axis=0)
    moe_rows = (moe_rows * slot_weights[:, None]).astype(bf16)
    hid = m2[:, :, slice_width:]
    hid = jnp.concatenate([hid[:, :, :cols], hid[:, :, cols:]], axis=1).reshape(all_rows, cols)
    lhs = jnp.concatenate([hid, onehot.T], axis=1)
    rhs = jnp.concatenate([dense_down, moe_rows], axis=0)
    block = jnp.dot(lhs, rhs, preferred_element_type=f32).astype(bf16)
    block = block.reshape(2, nzx, seqs, slice_width)
    from_other = other_core(block[1])
    block = (block[0].astype(f32) + from_other.astype(f32)).astype(bf16)
    combined = exchange(block, ZX).astype(f32).sum(axis=0)
    resid_own = lax.dynamic_slice_in_dim(resid, tp_start, slice_width, 1)
    return ((resid_own + combined).astype(bf16), new_keys, new_values)


def solution(mesh):
    shape = (mesh.shape["ep"] // 8, 4, 2, mesh.shape["tp"])
    split = Mesh(mesh.devices.reshape(shape), ("z", "x", "c", "tp"))
    return jax.shard_map(
        body,
        mesh=split,
        in_specs=(
            P(EP, None),
            P(),
            P(EP, "tp"),
            P(EP, "tp"),
            P(EP, "tp"),
            P("tp"),
            P(EP, "tp", None, None),
            P(EP, "tp", None, None),
            P(EP),
            P("tp", EP),
            P(),
            P(),
            P("tp", EP),
            P("tp", EP),
            P(EP, "tp"),
            P(EP, None),
            P(EP, None),
            P(EP, None, "tp"),
            P(EP, None, "tp"),
            P(EP, "tp", None),
        ),
        out_specs=(P(EP, "tp"), P(EP, "tp"), P(EP, "tp")),
        check_vma=False,
    )
```

```python
import functools
import jax
import jax.numpy as jnp
from jax import lax
from jax.experimental import pallas as pl
from jax.experimental.pallas import tpu as pltpu
from jax.sharding import Mesh
from jax.sharding import PartitionSpec as P

EP = ("z", "x", "c")
ZX = ("z", "x")

norm_eps = 1e-05
clamp_limit = 7.0
swish_alpha = 1.702
f32 = jnp.float32
bf16 = jnp.bfloat16
VM = pl.BlockSpec(memory_space=pltpu.VMEM)
SM = pl.BlockSpec(memory_space=pltpu.SMEM)

NX = 4


def rms_scale(values, gain):
    return values * lax.rsqrt(jnp.mean(values * values, axis=-1, keepdims=True) + norm_eps) * gain


def clamped_unit(gate_pre, up_pre):
    gate_c = jnp.minimum(gate_pre, clamp_limit)
    up_c = jnp.clip(up_pre, -clamp_limit, clamp_limit)
    return (up_c + 1.0) * gate_c * jax.nn.sigmoid(swish_alpha * gate_c)


def exchange(blocks, axes):
    return lax.all_to_all(blocks, axes, 0, 0, tiled=True)


def other_core(values):
    return lax.ppermute(values, "c", [(0, 1), (1, 0)])


def along_x(values, k):
    return lax.ppermute(values, "x", [(i, (i + k) % NX) for i in range(NX)])


def vmem(value):
    return pltpu.with_memory_space_constraint(value, pltpu.VMEM)


def local(kernel, name, outs, args, scratch=(), smem=0, keep=True, cost=None):
    multi = isinstance(outs, (list, tuple))
    if keep:
        outs = jax.tree.map(lambda s: pltpu.VMEM(s.shape, s.dtype), outs)
    args = tuple(args[:smem]) + tuple(vmem(a) for a in args[smem:])
    return pl.pallas_call(
        kernel,
        out_shape=outs,
        in_specs=[SM] * smem + [VM] * (len(args) - smem),
        out_specs=[VM] * len(outs) if multi else VM,
        scratch_shapes=list(scratch),
        compiler_params=pltpu.CompilerParams(vmem_limit_bytes=16 << 20),
        cost_estimate=cost,
        name=name,
    )(*args)


def sds(shape, dtype=bf16):
    return jax.ShapeDtypeStruct(tuple(shape), dtype)


def pick(parts, at):
    out = parts[0]
    for k in range(1, len(parts)):
        out = jnp.where(at == k, parts[k], out)
    return out


def prepare_kernel(nz, tok, gain, qw, kw, vw, owt, ids, rw, wcat, msg):
    qc, kc = qw.shape[1], kw.shape[1]
    wcat[:, :qc] = qw[...]
    wcat[:, qc : qc + kc] = kw[...]
    wcat[:, qc + kc :] = vw[...]
    normed = rms_scale(tok[...].astype(f32), gain[...]).astype(bf16)
    seqs = normed.shape[0]
    lane = lax.broadcasted_iota(jnp.int32, (seqs, 128), 1)
    hi = rw[...].astype(bf16).astype(f32)
    lo = rw[...] - hi
    idf = ids[...].astype(f32)
    top = idf.shape[1]
    meta = jnp.zeros((seqs, 128), f32)
    for k in range(top):
        meta = jnp.where(lane == k, idf[:, k : k + 1], meta)
        meta = jnp.where(lane == top + k, hi[:, k : k + 1], meta)
        meta = jnp.where(lane == 2 * top + k, lo[:, k : k + 1], meta)
    meta = meta.astype(bf16)
    heads = owt.shape[1]
    for z in range(nz):
        msg[z, :, :heads] = owt[...]
        msg[z, :seqs, heads : heads + 128] = meta
        msg[z, seqs:, heads : heads + 128] = meta
        msg[z, :seqs, heads + 128 :] = normed[:, z * 256 : z * 256 + 128]
        msg[z, seqs:, heads + 128 :] = normed[:, z * 256 + 128 : z * 256 + 256]


def project_kernel(at, got, w0, w1, w2, w3, wo, part, owm, w_s, f_s):
    x, c = at[1], at[2]
    nz, depth, wide = got.shape
    seqs = depth // 2
    for k, w in enumerate((w0, w1, w2, w3)):
        place = lax.rem(x + NX - k, NX) * 2
        w_s[pl.ds(pl.multiple_of((place + c) * depth, depth), depth)] = w[...]
        w_s[pl.ds(pl.multiple_of((place + 1 - c) * depth, depth), depth)] = wo[k]
    for z in range(nz):
        f_s[z * seqs : (z + 1) * seqs, :128] = got[z, :seqs, wide - 128 :]
        f_s[z * seqs : (z + 1) * seqs, 128:] = got[z, seqs:, wide - 128 :]
        owm[z] = got[z, :, : wide - 128]
    out = jnp.dot(f_s[...], w_s[...], preferred_element_type=f32).astype(bf16)
    for z in range(nz):
        part[z] = out[z * seqs : (z + 1) * seqs]


def attention_kernel(per_step, lengths, bias, part, k_ref, v_ref, att, nk, nv, q_s, a_s):
    seqs, _, span, head_dim = k_ref.shape
    heads = bias.shape[0]
    group = 8
    q_cols = heads * head_dim
    qkv = jnp.sum(part[...].astype(f32), axis=0)
    nk[...] = qkv[:, q_cols : q_cols + head_dim].astype(bf16)
    nv[...] = qkv[:, q_cols + head_dim :].astype(bf16)
    q_s[...] = jnp.zeros_like(q_s)
    for h in range(heads):
        q_s[:, h, :] = qkv[:, h * head_dim : (h + 1) * head_dim]

    rows = per_step * group
    row = lax.broadcasted_iota(jnp.int32, (rows, 1), 0)
    lane = lax.broadcasted_iota(jnp.int32, (rows, 128), 1)
    position = lax.broadcasted_iota(jnp.int32, (rows, span), 1)
    offset = jnp.zeros((rows, 1), f32)
    for h in range(heads):
        offset = jnp.where(row % group == h, bias[h], offset)

    @pl.loop(0, seqs // per_step)
    def _(step):
        scores = []
        length = jnp.zeros((rows, 1), jnp.int32)
        for i in range(per_step):
            q = q_s[step * per_step + i].astype(bf16)
            scores.append(
                lax.dot_general(
                    q,
                    k_ref[step * per_step + i, 0],
                    (((1,), (1,)), ((), ())),
                    preferred_element_type=f32,
                )
            )
            length = jnp.where(row // group == i, lengths[step * per_step + i], length)
        z = jnp.concatenate(scores, axis=0) * head_dim ** (-0.5) + offset
        inside = position < length
        tail = jnp.log1p(jnp.exp(-jnp.abs(z)))
        keep = jnp.where(inside, -jnp.maximum(z, 0.0) - tail, 0.0)
        take = jnp.minimum(z, 0.0) - tail
        chunks = span // 128
        after = jnp.zeros((rows, 1), f32)
        betweens = [None] * chunks
        for c in range(chunks - 1, -1, -1):
            own = keep[:, c * 128 : (c + 1) * 128]
            total = own
            shift = 1
            while shift < 128:
                moved = pltpu.roll(total, 128 - shift, 1)
                total = total + jnp.where(lane < 128 - shift, moved, 0.0)
                shift *= 2
            betweens[c] = total - own + after
            after = after + total[:, 0:1]
        between = jnp.concatenate(betweens, axis=1)
        weights = jnp.where(inside, jnp.exp(take + between), 0.0).astype(bf16)
        for i in range(per_step):
            a_s[step * per_step + i] = jnp.dot(
                weights[i * group : (i + 1) * group],
                v_ref[step * per_step + i, 0],
                preferred_element_type=f32,
            )

    for h in range(heads):
        att[:, h * head_dim : (h + 1) * head_dim] = a_s[:, h, :].astype(bf16)


def mix_kernel(at, att, *refs):
    mine, others, msg, w_s = refs[:NX], refs[NX : 2 * NX], refs[2 * NX], refs[2 * NX + 1]
    x, c = at[1], at[2]
    nz, depth = mine[0].shape[:2]
    heads = att.shape[1]
    for k in range(NX):
        place = lax.rem(x + NX - k, NX) * 2
        for z in range(nz):
            base = z * NX * 2
            w_s[pl.ds(pl.multiple_of((base + place + c) * depth, depth), depth)] = mine[k][
                z, :, :heads
            ]
            w_s[pl.ds(pl.multiple_of((base + place + 1 - c) * depth, depth), depth)] = others[k][
                z, :, :heads
            ]
    out = lax.dot_general(
        att[...], w_s[...], (((1,), (1,)), ((), ())), preferred_element_type=f32
    ).astype(bf16)
    for t in range(msg.shape[0]):
        msg[t] = out


def slots_kernel(seqs, heads, top, at, *refs):
    pieces = refs[: 2 * NX]
    pickm, him, lom, m_s = refs[2 * NX :]
    x = at[1]
    nz = pieces[0].shape[0]
    half = nz * NX * seqs
    for r in range(2):
        for k in range(NX):
            place = lax.rem(x + NX - k, NX) * seqs
            for z in range(nz):
                start = pl.multiple_of(r * half + z * NX * seqs + place, seqs)
                m_s[pl.ds(start, seqs)] = pieces[r * NX + k][z, :seqs, heads : heads + 128]
    expert = (at[0] * NX + x) * 2 + at[2]
    m = m_s[...].astype(f32)
    rows = m.shape[0]
    lane = lax.broadcasted_iota(jnp.int32, (rows, 128), 1)
    row = lax.broadcasted_iota(jnp.int32, (rows, 128), 0)
    hit = jnp.where((m == expert.astype(f32)) & (lane < top), 1.0, 0.0)
    hi = jnp.sum(hit * pltpu.roll(m, 128 - top, 1), axis=1, keepdims=True)
    lo = jnp.sum(hit * pltpu.roll(m, 128 - 2 * top, 1), axis=1, keepdims=True)
    own = jnp.broadcast_to(jnp.sum(hit, axis=1, keepdims=True), (rows, 128))
    upto = own
    shift = 1
    while shift < seqs:
        upto = upto + jnp.where(row % seqs >= shift, pltpu.roll(upto, shift, 0), 0.0)
        shift *= 2
    slot = (row // seqs) * 2 + (upto - own).astype(jnp.int32)
    here = jnp.where((lane == slot) & (own > 0.5), 1.0, 0.0)
    pickm[...] = here.astype(bf16)
    him[...] = (here * hi).astype(bf16)
    lom[...] = (here * lo).astype(bf16)


def norm_kernel(at, got, tok, gain, msg, res):
    t = at[3]
    mixed = jnp.sum(got[...].astype(f32), axis=0).astype(bf16).astype(f32)
    resid = tok[...].astype(f32) + mixed
    normed = rms_scale(resid, gain[...])
    wide = msg.shape[2]
    parts = resid.shape[1] // wide
    res[...] = pick([resid[:, k * wide : (k + 1) * wide] for k in range(parts)], t)
    own = pick([normed[:, k * wide : (k + 1) * wide] for k in range(parts)], t).astype(bf16)
    for b in range(msg.shape[0]):
        msg[b] = own


def spread_kernel(at, mine, other, dg, du, bg, pickm, msg, x_s, w_s):
    t = at[3]
    nb, seqs, wide = mine.shape
    half = nb * seqs
    cols = dg.shape[1]
    x_s[:half] = mine[...].reshape(half, wide)
    x_s[half:] = other[...].reshape(half, wide)
    w_s[:, :cols] = dg[...]
    w_s[:, cols:] = du[...]
    x = x_s[...]
    pre = jnp.dot(x, w_s[...], preferred_element_type=f32).astype(bf16)
    gate = pick([bg[:, k * wide : (k + 1) * wide] for k in range(bg.shape[1] // wide)], t)
    gate = jnp.broadcast_to(gate.astype(f32), (16, wide)).astype(bf16)
    branch = lax.dot_general(
        gate, x, (((1,), (1,)), ((), ())), preferred_element_type=f32
    ).astype(bf16)
    rows = lax.dot_general(
        pickm[...], x, (((0,), (0,)), ((), ())), preferred_element_type=f32
    ).astype(bf16)
    nt = msg.shape[0]
    quarter = 2 * half // nt
    slots = rows.shape[0]
    fold = wide // 2
    for q in range(nt):
        msg[q, :quarter, :fold] = pre[q * quarter : (q + 1) * quarter]
        msg[q, :slots, fold:] = rows[:, :fold]
        msg[q, slots:quarter, fold:] = rows[:, fold:]
        msg[q, quarter:, :fold] = branch[:, q * quarter : (q + 1) * quarter]
        msg[q, quarter:, fold:] = branch[:, q * quarter : (q + 1) * quarter]


def expert_kernel(got, eg, eu, ed, msg):
    nt, rows, wide = got.shape
    quarter = rows - 16
    fold = wide // 2
    slots = quarter // 2
    gate_pre = up_pre = None
    for t in range(nt):
        x = jnp.concatenate([got[t, :slots, fold:], got[t, slots:quarter, fold:]], axis=1)
        g = jnp.dot(x, eg[0, t * wide : (t + 1) * wide], preferred_element_type=f32)
        u = jnp.dot(x, eu[0, t * wide : (t + 1) * wide], preferred_element_type=f32)
        gate_pre = g if gate_pre is None else gate_pre + g
        up_pre = u if up_pre is None else up_pre + u
    act = clamped_unit(gate_pre, up_pre).astype(bf16)
    out = jnp.dot(act, ed[0], preferred_element_type=f32).astype(bf16)
    pre = jnp.sum(got[:, :quarter, :fold].astype(f32), axis=0)
    cols = fold // 2
    branch = jnp.sum(got[:, quarter : quarter + 16, :fold].astype(f32), axis=0)[0:1]
    r = lax.broadcasted_iota(jnp.int32, (quarter, quarter), 0)
    c = lax.broadcasted_iota(jnp.int32, (quarter, quarter), 1)
    branch = jnp.sum(jnp.where(r == c, branch, 0.0), axis=1, keepdims=True)
    hidden = jax.nn.silu(pre[:, :cols]) * pre[:, cols:] * jax.nn.sigmoid(branch)
    hidden = hidden.astype(bf16)
    for t in range(nt):
        msg[t, :, :wide] = out[:, t * wide : (t + 1) * wide]
        msg[t, :, wide : wide + cols] = hidden[:slots]
        msg[t, :, wide + cols :] = hidden[slots:]


def block_kernel(which, got, dd, him, lom, out):
    nt, slots, wide = got.shape
    cols = dd.shape[0]
    wide = wide - 2 * cols
    rows = jnp.sum(got[:, :, :wide].astype(f32), axis=0).astype(bf16)
    half = out.shape[0] * out.shape[1]
    hidden = []
    for q in range(which * nt // 2, (which + 1) * nt // 2):
        hidden.append(got[q, :, wide : wide + cols])
        hidden.append(got[q, :, wide + cols :])
    left = jnp.concatenate(
        [
            jnp.concatenate(hidden, axis=0),
            him[which * half : (which + 1) * half],
            lom[which * half : (which + 1) * half],
        ],
        axis=1,
    )
    right = jnp.concatenate([dd[...], rows, rows], axis=0)
    full = jnp.dot(left, right, preferred_element_type=f32)
    out[...] = full.astype(out.dtype).reshape(out.shape)


def add_kernel(a, b, out):
    out[...] = (a[...] + b[...].astype(f32)).astype(bf16)


def final_kernel(got, res, out):
    out[...] = (jnp.sum(got[...].astype(f32), axis=0) + res[...]).astype(bf16)


def body(
    tokens,
    attn_gain,
    query_weight,
    key_weight,
    value_weight,
    break_bias,
    cache_keys,
    cache_values,
    lengths,
    out_weight,
    ffn_gain,
    branch_gate,
    dense_gate,
    dense_up,
    dense_down,
    route_ids,
    route_weights,
    expert_gate,
    expert_up,
    expert_down,
):
    nz, nt = lax.axis_size("z"), lax.axis_size("tp")
    nzx = nz * NX
    seqs, width = tokens.shape
    top = route_ids.shape[1]
    slice_width = width // nt
    all_rows = 2 * nzx * seqs
    slots = 2 * nzx * 2
    depth = query_weight.shape[0]
    heads = out_weight.shape[0]
    proj = query_weight.shape[1] + 2 * key_weight.shape[1]
    at = jnp.stack([lax.axis_index(a) for a in ("z", "x", "c", "tp")]).astype(jnp.int32)

    busy = pl.CostEstimate(flops=20_000_000_000, transcendentals=0, bytes_accessed=1 << 20)
    wcat, msg = local(
        functools.partial(prepare_kernel, nz),
        "prepare",
        [sds((depth, proj)), sds((nz, depth, heads + 256))],
        (
            tokens,
            attn_gain[None],
            query_weight,
            key_weight,
            value_weight,
            out_weight.T,
            route_ids,
            route_weights,
        ),
    )
    got = exchange(msg, "z")
    w_x = [wcat] + [along_x(wcat, k) for k in range(1, NX)]
    w_other = other_core(jnp.stack(w_x))
    part, owm = local(
        project_kernel,
        "project",
        [sds((nz, seqs, proj)), sds((nz, depth, heads + 128))],
        (at, got, *w_x, w_other),
        [pltpu.VMEM((2 * NX * depth, proj), bf16), pltpu.VMEM((nz * seqs, 2 * NX * depth), bf16)],
        smem=1,
        cost=busy,
    )
    part = exchange(part, "z")
    ow = [owm] + [along_x(owm, k) for k in range(1, NX)]
    ow_other = [other_core(piece) for piece in ow]

    head_dim = cache_keys.shape[3]
    attended, new_keys, new_values = local(
        functools.partial(attention_kernel, 4),
        "attention",
        [sds((seqs, heads)), sds((seqs, head_dim)), sds((seqs, head_dim))],
        (lengths, break_bias, part, cache_keys, cache_values),
        [pltpu.VMEM((seqs, 8, head_dim), f32)] * 2,
        smem=2,
    )

    msg = local(
        mix_kernel,
        "mix",
        sds((nt, seqs, width)),
        (at, attended, *ow, *ow_other),
        [pltpu.VMEM((width, heads), bf16)],
        smem=1,
    )
    mixed = exchange(msg, "tp")
    pickm, him, lom = local(
        functools.partial(slots_kernel, seqs, heads, top),
        "slots",
        [sds((all_rows, slots))] * 3,
        (at, *ow, *ow_other),
        [pltpu.VMEM((all_rows, 128), bf16)],
        smem=1,
    )
    msg, resid = local(
        norm_kernel,
        "norm",
        [sds((nzx, seqs, slice_width)), sds((seqs, slice_width), f32)],
        (at, mixed, tokens, ffn_gain[None]),
        smem=1,
    )
    mine = exchange(msg, ZX)
    other = other_core(mine)
    cols = dense_gate.shape[1]
    msg = local(
        spread_kernel,
        "spread",
        sds((nt, all_rows // nt + 16, slice_width)),
        (at, mine, other, dense_gate, dense_up, branch_gate[None], pickm),
        [pltpu.VMEM((all_rows, slice_width), bf16), pltpu.VMEM((slice_width, 2 * cols), bf16)],
        smem=1,
    )
    got = exchange(msg, "tp")
    msg = local(
        expert_kernel,
        "expert",
        sds((nt, slots, slice_width + 2 * cols)),
        (got, expert_gate, expert_up, expert_down),
    )
    got = exchange(msg, "tp")
    parts = (got, dense_down, him, lom)
    shape = (nzx, seqs, slice_width)
    sent = local(functools.partial(block_kernel, 1), "block_other", sds(shape), parts)
    arrived = other_core(sent)
    kept = local(functools.partial(block_kernel, 0), "block_mine", sds(shape, f32), parts)
    block = local(add_kernel, "add", sds(shape), (kept, arrived))
    got = exchange(block, ZX)
    out = local(final_kernel, "final", sds((seqs, slice_width)), (got, resid), keep=False)
    return out, new_keys, new_values


def solution(mesh):
    shape = (mesh.shape["ep"] // (2 * NX), NX, 2, mesh.shape["tp"])
    split = Mesh(mesh.devices.reshape(shape), ("z", "x", "c", "tp"))
    return jax.shard_map(
        body,
        mesh=split,
        in_specs=(
            P(EP, None),
            P(),
            P(EP, "tp"),
            P(EP, "tp"),
            P(EP, "tp"),
            P("tp"),
            P(EP, "tp", None, None),
            P(EP, "tp", None, None),
            P(EP),
            P("tp", EP),
            P(),
            P(),
            P("tp", EP),
            P("tp", EP),
            P(EP, "tp"),
            P(EP, None),
            P(EP, None),
            P(EP, None, "tp"),
            P(EP, None, "tp"),
            P(EP, "tp", None),
        ),
        out_specs=(P(EP, "tp"), P(EP, "tp"), P(EP, "tp")),
        check_vma=False,
    )
```

```python
import functools
import jax
import jax.numpy as jnp
from jax import lax
from jax.experimental import pallas as pl
from jax.experimental.pallas import tpu as pltpu
from jax.sharding import Mesh
from jax.sharding import PartitionSpec as P

EP = ("z", "x", "c")
ZX = ("z", "x")

norm_eps = 1e-05
clamp_limit = 7.0
swish_alpha = 1.702
f32 = jnp.float32
bf16 = jnp.bfloat16
VM = pl.BlockSpec(memory_space=pltpu.VMEM)
SM = pl.BlockSpec(memory_space=pltpu.SMEM)

NX = 4


def rms_scale(values, gain):
    return values * lax.rsqrt(jnp.mean(values * values, axis=-1, keepdims=True) + norm_eps) * gain


def clamped_unit(gate_pre, up_pre):
    gate_c = jnp.minimum(gate_pre, clamp_limit)
    up_c = jnp.clip(up_pre, -clamp_limit, clamp_limit)
    return (up_c + 1.0) * gate_c * jax.nn.sigmoid(swish_alpha * gate_c)


def exchange(blocks, axes):
    return lax.all_to_all(blocks, axes, 0, 0, tiled=True)


def other_core(values):
    return lax.ppermute(values, "c", [(0, 1), (1, 0)])


def along_x(values, k):
    return lax.ppermute(values, "x", [(i, (i + k) % NX) for i in range(NX)])


def local(kernel, name, outs, args, scratch=(), smem=0, keep=True, pin=pltpu.VMEM):
    multi = isinstance(outs, (list, tuple))
    if keep:
        outs = jax.tree.map(lambda s: pltpu.VMEM(s.shape, s.dtype), outs)
    pins = pin if isinstance(pin, tuple) else (pin,) * (len(args) - smem)
    args = tuple(args[:smem]) + tuple(
        pltpu.with_memory_space_constraint(a, p) for a, p in zip(args[smem:], pins)
    )
    return pl.pallas_call(
        kernel,
        out_shape=outs,
        in_specs=[SM] * smem + [VM] * (len(args) - smem),
        out_specs=[VM] * len(outs) if multi else VM,
        scratch_shapes=list(scratch),
        compiler_params=pltpu.CompilerParams(vmem_limit_bytes=16 << 20),
        name=name,
    )(*args)


def sds(shape, dtype=bf16):
    return jax.ShapeDtypeStruct(tuple(shape), dtype)


def pick(parts, at):
    out = parts[0]
    for k in range(1, len(parts)):
        out = jnp.where(at == k, parts[k], out)
    return out


def prepare_kernel(nz, tok, gain, qw, kw, vw, owt, ids, rw, wcat, msg):
    qc, kc = qw.shape[1], kw.shape[1]
    proj = qc + 2 * kc
    wcat[:, :qc] = qw[...]
    wcat[:, qc : qc + kc] = kw[...]
    wcat[:, qc + kc : proj] = vw[...]
    normed = rms_scale(tok[...].astype(f32), gain[...]).astype(bf16)
    seqs = normed.shape[0]
    lane = lax.broadcasted_iota(jnp.int32, (seqs, 128), 1)
    row = lax.broadcasted_iota(jnp.int32, (seqs, seqs), 0)
    col = lax.broadcasted_iota(jnp.int32, (seqs, seqs), 1)
    hi = rw[...].astype(bf16).astype(f32)
    lo = rw[...] - hi
    idf = ids[...].astype(f32)
    top = idf.shape[0]
    meta = jnp.zeros((seqs, 128), f32)
    for j, values in enumerate((idf, hi, lo)):
        for k in range(top):
            down = jnp.sum(jnp.where(row == col, values[k : k + 1], 0.0), axis=1, keepdims=True)
            meta = jnp.where(lane == j * top + k, down, meta)
    meta = meta.astype(bf16)
    wcat[:seqs, proj:] = meta
    wcat[seqs:, proj:] = jnp.zeros((wcat.shape[0] - seqs, 128), bf16)
    heads = owt.shape[1]
    for z in range(nz):
        msg[z, :, :heads] = owt[...]
        msg[z, :seqs, heads:] = normed[:, z * 256 : z * 256 + 128]
        msg[z, seqs:, heads:] = normed[:, z * 256 + 128 : z * 256 + 256]


def project_kernel(at, got, w0, w1, w2, w3, wo, part, owm, w_s, f_s):
    x, c = at[1], at[2]
    nz, depth, wide = got.shape
    seqs = depth // 2
    proj = w_s.shape[1]
    table = jnp.zeros((seqs, 128), f32)
    for k, w in enumerate((w0, w1, w2, w3)):
        place = lax.rem(x + NX - k, NX) * 2
        w_s[pl.ds(pl.multiple_of((place + c) * depth, depth), depth)] = w[:, :proj]
        w_s[pl.ds(pl.multiple_of((place + 1 - c) * depth, depth), depth)] = wo[k, :, :proj]
        table += pltpu.roll(w[:seqs, proj:].astype(f32), k * 16, 1)
        table += pltpu.roll(wo[k, :seqs, proj:].astype(f32), (NX + k) * 16, 1)
    table = table.astype(bf16)
    for z in range(nz):
        f_s[z * seqs : (z + 1) * seqs, :128] = got[z, :seqs, wide - 128 :]
        f_s[z * seqs : (z + 1) * seqs, 128:] = got[z, seqs:, wide - 128 :]
        owm[z] = got[z, :, : wide - 128]
    out = jnp.dot(f_s[...], w_s[...], preferred_element_type=f32).astype(bf16)
    for z in range(nz):
        part[z, :, :proj] = out[z * seqs : (z + 1) * seqs]
        part[z, :, proj:] = table


def attention_kernel(
    block, lengths, bias, part, k_hbm, v_hbm, att, nk, nv, k_ref, v_ref, q_s, z_s, w_s, sems
):
    seqs, _, span, head_dim = k_ref.shape
    piece = 256
    steps = span // piece
    pairs = ((k_hbm, k_ref), (v_hbm, v_ref))

    def each_size(which, s, act):
        live = lax.div(lengths[s] + piece - 1, piece)
        for n in range(1, steps + 1):

            @pl.when(live == n)
            def _():
                place = (s, 0, pl.ds(0, n * piece))
                source, target = pairs[which]
                act(
                    pltpu.make_async_copy(source.at[place], target.at[place], sems.at[which, s]), n
                )

    def begin(copy, n):
        copy.start()

    @pl.loop(0, seqs)
    def _(s):
        each_size(0, s, begin)

    @pl.loop(0, seqs)
    def _(s):
        def clear(copy, n):
            copy.start()
            if n < steps:
                rest = (steps - n) * piece
                v_ref[s, 0, pl.ds(n * piece, rest)] = jnp.zeros((rest, head_dim), bf16)

        each_size(1, s, clear)

    heads = bias.shape[0]
    q_cols = heads * head_dim
    both = 2 * heads
    qkv = jnp.sum(part[:, :, : q_cols + 2 * head_dim].astype(f32), axis=0)
    nk[...] = qkv[:, q_cols : q_cols + head_dim].astype(bf16)
    nv[...] = qkv[:, q_cols + head_dim :].astype(bf16)
    for s in range(seqs):
        for h in range(heads):
            at_row = s * heads + h
            q_s[at_row : at_row + 1] = qkv[s : s + 1, h * head_dim : (h + 1) * head_dim]

    upper = lax.broadcasted_iota(jnp.int32, (both, 1), 0) < heads

    def wait(copy, n):
        copy.wait()

    @pl.loop(0, seqs // 2)
    def _(i):
        s = i * 2
        each_size(0, s, wait)
        each_size(0, s + 1, wait)
        here = pl.ds(pl.multiple_of(s * heads, both), both)
        q = q_s[here].astype(bf16)
        pair = [
            lax.dot_general(
                q, k_ref[s + j, 0], (((1,), (1,)), ((), ())), preferred_element_type=f32
            )
            for j in range(2)
        ]
        z_s[here] = jnp.where(upper, pair[0], pair[1])

    rows = block * heads
    row = lax.broadcasted_iota(jnp.int32, (rows, 1), 0)
    lane = lax.broadcasted_iota(jnp.int32, (rows, 128), 1)
    offset = jnp.zeros((rows, 1), f32)
    for h in range(heads):
        offset = jnp.where(row % heads == h, bias[h], offset)
    chunks = span // 128

    @pl.loop(0, seqs // block)
    def _(step):
        length = jnp.zeros((rows, 1), jnp.int32)
        for i in range(block):
            length = jnp.where(row // heads == i, lengths[step * block + i], length)
        here = pl.ds(pl.multiple_of(step * rows, rows), rows)
        after = jnp.zeros((rows, 1), f32)
        for c in range(chunks - 1, -1, -1):
            cols = slice(c * 128, (c + 1) * 128)
            z = z_s[here, cols] * head_dim ** (-0.5) + offset
            inside = lane + c * 128 < length
            tail = jnp.log1p(jnp.exp(-jnp.abs(z)))
            keep = jnp.where(inside, -jnp.maximum(z, 0.0) - tail, 0.0)
            total = keep
            shift = 1
            while shift < 128:
                moved = pltpu.roll(total, 128 - shift, 1)
                total = total + jnp.where(lane < 128 - shift, moved, 0.0)
                shift *= 2
            between = total - keep + after
            after = after + total[:, 0:1]
            power = jnp.exp(jnp.minimum(z, 0.0) - tail + between)
            w_s[here, cols] = jnp.where(inside, power, 0.0)

    @pl.loop(0, seqs // 2)
    def _(i):
        s = i * 2
        each_size(1, s, wait)
        each_size(1, s + 1, wait)
        here = pl.ds(pl.multiple_of(s * heads, both), both)
        w = w_s[here].astype(bf16)
        pair = [jnp.dot(w, v_ref[s + j, 0], preferred_element_type=f32) for j in range(2)]
        q_s[here] = jnp.where(upper, pair[0], pair[1])

    out = q_s[...].astype(bf16).astype(f32)
    for s in range(seqs):
        for h in range(heads):
            at_row = s * heads + h
            att[s : s + 1, h * head_dim : (h + 1) * head_dim] = out[at_row : at_row + 1].astype(
                bf16
            )


def attention(part, bias, keys, values, lengths):
    seqs, _, span, head_dim = keys.shape
    heads = bias.shape[0]
    outs = [sds((seqs, heads * head_dim)), sds((seqs, head_dim)), sds((seqs, head_dim))]
    hbm = pl.BlockSpec(memory_space=pltpu.HBM)
    pins = (pltpu.VMEM, pltpu.HBM, pltpu.HBM)
    args = [
        pltpu.with_memory_space_constraint(a, p) for a, p in zip((part, keys, values), pins)
    ]
    return pl.pallas_call(
        functools.partial(attention_kernel, 8),
        out_shape=outs,
        in_specs=[SM, SM, VM, hbm, hbm],
        out_specs=[VM] * 3,
        scratch_shapes=[pltpu.VMEM(keys.shape, bf16)] * 2
        + [pltpu.VMEM((seqs * heads, head_dim), f32)]
        + [pltpu.VMEM((seqs * heads, span), f32)] * 2
        + [pltpu.SemaphoreType.DMA((2, seqs))],
        compiler_params=pltpu.CompilerParams(vmem_limit_bytes=24 << 20),
        name="attention",
    )(*(pltpu.with_memory_space_constraint(a, pltpu.HBM) for a in (lengths, bias)), *args)


def mix_kernel(at, att, *refs):
    mine, others, msg, w_s = refs[:NX], refs[NX : 2 * NX], refs[2 * NX], refs[2 * NX + 1]
    x, c = at[1], at[2]
    nz, depth = mine[0].shape[:2]
    heads = att.shape[1]
    for k in range(NX):
        place = lax.rem(x + NX - k, NX) * 2
        for z in range(nz):
            base = z * NX * 2
            w_s[pl.ds(pl.multiple_of((base + place + c) * depth, depth), depth)] = mine[k][
                z, :, :heads
            ]
            w_s[pl.ds(pl.multiple_of((base + place + 1 - c) * depth, depth), depth)] = others[k][
                z, :, :heads
            ]
    out = lax.dot_general(
        att[...], w_s[...], (((1,), (1,)), ((), ())), preferred_element_type=f32
    ).astype(bf16)
    for t in range(msg.shape[0]):
        msg[t] = out


def slots_kernel(seqs, top, at, part, him, lom, m_s):
    x = at[1]
    nz, _, wide = part.shape
    half = nz * NX * seqs
    for z in range(nz):
        table = part[z, :, wide - 128 :].astype(f32)
        for r in range(2):
            for k in range(NX):
                place = lax.rem(x + NX - k, NX) * seqs
                start = pl.multiple_of(r * half + z * NX * seqs + place, seqs)
                shift = (r * NX + k) * 16
                m_s[pl.ds(start, seqs)] = pltpu.roll(table, (128 - shift) % 128, 1)
    expert = (at[0] * NX + x) * 2 + at[2]
    m = m_s[...]
    rows = m.shape[0]
    lane = lax.broadcasted_iota(jnp.int32, (rows, 128), 1)
    row = lax.broadcasted_iota(jnp.int32, (rows, 128), 0)
    hit = jnp.where((m == expert.astype(f32)) & (lane < top), 1.0, 0.0)
    hi = jnp.sum(hit * pltpu.roll(m, 128 - top, 1), axis=1, keepdims=True)
    lo = jnp.sum(hit * pltpu.roll(m, 128 - 2 * top, 1), axis=1, keepdims=True)
    own = jnp.broadcast_to(jnp.sum(hit, axis=1, keepdims=True), (rows, 128))
    upto = own
    shift = 1
    while shift < seqs:
        upto = upto + jnp.where(row % seqs >= shift, pltpu.roll(upto, shift, 0), 0.0)
        shift *= 2
    slot = (row // seqs) * 2 + (upto - own).astype(jnp.int32)
    here = jnp.where((lane == slot) & (own > 0.5), 1.0, 0.0)
    him[...] = (here * hi).astype(bf16)
    lom[...] = (here * lo).astype(bf16)


def norm_kernel(at, got, tok, gain, ids, msg, res):
    t = at[3]
    mixed = jnp.sum(got[...].astype(f32), axis=0).astype(bf16).astype(f32)
    resid = tok[...].astype(f32) + mixed
    normed = rms_scale(resid, gain[...]).astype(bf16)
    seqs, width = resid.shape
    nb, share, _ = msg.shape
    parts = got.shape[0]
    wide = width // parts
    own = share // 2
    res[...] = pick([resid[:, k * wide : (k + 1) * wide] for k in range(parts)], t)
    top = ids.shape[0]
    experts = 2 * nb
    expert = lax.broadcasted_iota(jnp.int32, (experts, seqs), 0)
    hit = jnp.zeros((experts, seqs), f32)
    for k in range(top):
        hit = jnp.where(ids[k : k + 1] == expert, 1.0, hit)
    lane = lax.broadcasted_iota(jnp.int32, (seqs, seqs), 1)
    before = jnp.where(lax.broadcasted_iota(jnp.int32, (seqs, seqs), 0) < lane, 1.0, 0.0)
    rank = jnp.dot(hit, before, preferred_element_type=f32)
    quarter = lax.broadcasted_iota(jnp.int32, (own, seqs), 0) + t * own
    quarter = jnp.where(quarter == lax.broadcasted_iota(jnp.int32, (own, seqs), 1), 1.0, 0.0)
    first = jnp.where(rank < 0.5, hit, 0.0)
    second = jnp.where(rank > 0.5, hit, 0.0)
    choose = []
    for b in range(nb):
        choose.append(quarter)
        for c in range(2):
            e = 2 * b + c
            choose.append(first[e : e + 1])
            choose.append(second[e : e + 1])
    choose = jnp.concatenate(choose, axis=0).astype(bf16)
    rows = jnp.dot(choose, normed, preferred_element_type=f32).astype(bf16)
    msg[...] = rows.reshape(msg.shape)


def expert_kernel(
    at, mine, other, w0, w1, w2, w3, bg, eg, eu, ed, msg, w_s, d_s, x_s, r_s, sems
):
    t = at[3]
    nb, share, width = mine.shape
    own = share // 2
    nt, slots, _ = msg.shape
    wide = width // nt
    cols = w0.shape[1] // 2
    copies = [pltpu.make_async_copy(ed.at[0], d_s, sems.at[nt])]
    for k, w in enumerate((w0, w1, w2, w3)):
        place = pl.multiple_of(lax.rem(t + nt - k, nt) * wide, wide)
        copies.append(pltpu.make_async_copy(w, w_s.at[pl.ds(place, wide)], sems.at[k]))
    for copy in copies:
        copy.start()
    core = at[2]
    half = nb * own
    for h, part in enumerate((mine, other)):
        block = part[...].astype(f32)
        routed = jnp.where(core == 0, block[:, own : own + 2], block[:, own + 2 :])
        r_s[h * 2 * nb : (h + 1) * 2 * nb] = routed.reshape(2 * nb, width).astype(bf16)
        x_s[h * half : (h + 1) * half] = block[:, :own].reshape(half, width).astype(bf16)
    rows = r_s[...]
    gate_pre = jnp.dot(rows, eg[0], preferred_element_type=f32)
    up_pre = jnp.dot(rows, eu[0], preferred_element_type=f32)
    act = clamped_unit(gate_pre, up_pre).astype(bf16)
    copies[0].wait()
    out = jnp.dot(act, d_s[...], preferred_element_type=f32).astype(bf16)
    for q in range(nt):
        msg[q, :, :wide] = out[:, q * wide : (q + 1) * wide]
    x = x_s[...]
    gate = jnp.broadcast_to(bg[...].astype(f32), (8, width)).astype(bf16)
    branch = lax.dot_general(x, gate, (((1,), (1,)), ((), ())), preferred_element_type=f32)
    for copy in copies[1:]:
        copy.wait()
    pre = jnp.dot(x, w_s[...], preferred_element_type=f32)
    hidden = jax.nn.silu(pre[:, :cols]) * pre[:, cols:] * jax.nn.sigmoid(branch[:, 0:1])
    hidden = hidden.astype(bf16)
    for q in range(nt):
        msg[q, :, wide : wide + cols] = hidden[:slots]
        msg[q, :, wide + cols :] = hidden[slots:]


def block_kernel(which, got, dd, him, lom, out, h_s):
    nt, slots, wide = got.shape
    cols = dd.shape[0]
    wide = wide - 2 * cols
    rows = jnp.sum(got[:, :, :wide].astype(f32), axis=0).astype(bf16)
    nb, seqs, _ = out.shape
    half = nb * seqs
    own = seqs // nt
    start = wide + which * cols
    for q in range(nt):
        part = got[q, :, start : start + cols].astype(f32)
        h_s[:, q * own : (q + 1) * own] = part.reshape(nb, own, cols)
    left = jnp.concatenate(
        [
            h_s[...].reshape(half, cols).astype(bf16),
            him[which * half : (which + 1) * half],
            lom[which * half : (which + 1) * half],
        ],
        axis=1,
    )
    right = jnp.concatenate([dd[...], rows, rows], axis=0)
    full = jnp.dot(left, right, preferred_element_type=f32)
    out[...] = full.astype(out.dtype).reshape(out.shape)


def add_kernel(a, b, out):
    out[...] = (a[...] + b[...].astype(f32)).astype(bf16)


def final_kernel(got, res, out):
    out[...] = (jnp.sum(got[...].astype(f32), axis=0) + res[...]).astype(bf16)


def body(
    tokens,
    attn_gain,
    query_weight,
    key_weight,
    value_weight,
    break_bias,
    cache_keys,
    cache_values,
    lengths,
    out_weight,
    ffn_gain,
    branch_gate,
    dense_gate,
    dense_up,
    dense_down,
    route_ids,
    route_weights,
    expert_gate,
    expert_up,
    expert_down,
):
    nz, nt = lax.axis_size("z"), lax.axis_size("tp")
    nzx = nz * NX
    seqs, width = tokens.shape
    top = route_ids.shape[1]
    slice_width = width // nt
    all_rows = 2 * nzx * seqs
    slots = 2 * nzx * 2
    depth = query_weight.shape[0]
    heads = out_weight.shape[0]
    proj = query_weight.shape[1] + 2 * key_weight.shape[1]
    at = jnp.stack([lax.axis_index(a) for a in ("z", "x", "c", "tp")]).astype(jnp.int32)

    wcat, msg = local(
        functools.partial(prepare_kernel, nz),
        "prepare",
        [sds((depth, proj + 128)), sds((nz, depth, heads + 128))],
        (
            tokens,
            attn_gain[None],
            query_weight,
            key_weight,
            value_weight,
            out_weight.T,
            route_ids.T,
            route_weights.T,
        ),
        pin=pltpu.HBM,
    )
    with jax.named_scope("over_z"):
        got = exchange(msg, "z")
    with jax.named_scope("weights_x"):
        w_x = [wcat] + [along_x(wcat, k) for k in range(1, NX)]
    w_other = other_core(jnp.stack(w_x))
    part, owm = local(
        project_kernel,
        "project",
        [sds((nz, seqs, proj + 128)), sds((nz, depth, heads))],
        (at, got, *w_x, w_other),
        [pltpu.VMEM((2 * NX * depth, proj), bf16), pltpu.VMEM((nz * seqs, 2 * NX * depth), bf16)],
        smem=1,
    )
    with jax.named_scope("partial_z"):
        part = exchange(part, "z")
    with jax.named_scope("mix_x"):
        ow = [owm] + [along_x(owm, k) for k in range(1, NX)]
    ow_other = [other_core(piece) for piece in ow]

    attended, new_keys, new_values = attention(
        part, break_bias, cache_keys, cache_values, lengths
    )

    msg = local(
        mix_kernel,
        "mix",
        sds((nt, seqs, width)),
        (at, attended, *ow, *ow_other),
        [pltpu.VMEM((width, heads), bf16)],
        smem=1,
    )
    mixed = exchange(msg, "tp")
    him, lom = local(
        functools.partial(slots_kernel, seqs, top),
        "slots",
        [sds((all_rows, slots))] * 2,
        (at, part),
        [pltpu.VMEM((all_rows, 128), f32)],
        smem=1,
    )
    own = seqs // nt
    cols = dense_gate.shape[1]
    msg, resid = local(
        norm_kernel,
        "norm",
        [sds((nzx, 2 * own, width)), sds((seqs, slice_width), f32)],
        (at, mixed, tokens, ffn_gain[None], route_ids.T),
        smem=1,
    )
    with jax.named_scope("rows_zx"):
        mine = exchange(msg, ZX)
    with jax.named_scope("dense_tp"):
        gu = jnp.concatenate([dense_gate, dense_up], axis=1)
        gu = [gu] + [
            lax.ppermute(gu, "tp", [(i, (i + k) % nt) for i in range(nt)]) for k in range(1, nt)
        ]
    mine, *gu = lax.optimization_barrier((mine, *gu))
    other, him, lom = lax.optimization_barrier((other_core(mine), him, lom))
    hbm = pl.BlockSpec(memory_space=pltpu.HBM)
    places = [pltpu.VMEM] * 2 + [pltpu.HBM] * nt + [pltpu.VMEM] * 3 + [pltpu.HBM]
    operands = (mine, other, *gu, branch_gate[None], expert_gate, expert_up, expert_down)
    msg = pl.pallas_call(
        expert_kernel,
        out_shape=pltpu.VMEM((nt, slots, slice_width + 2 * cols), bf16),
        in_specs=[SM] + [hbm if p == pltpu.HBM else VM for p in places],
        out_specs=VM,
        scratch_shapes=[
            pltpu.VMEM((width, 2 * cols), bf16),
            pltpu.VMEM(expert_down.shape[1:], bf16),
            pltpu.VMEM((2 * nzx * own, width), bf16),
            pltpu.VMEM((slots, width), bf16),
            pltpu.SemaphoreType.DMA((nt + 1,)),
        ],
        compiler_params=pltpu.CompilerParams(vmem_limit_bytes=16 << 20),
        name="expert",
    )(at, *(pltpu.with_memory_space_constraint(a, p) for a, p in zip(operands, places)))
    got = exchange(msg, "tp")
    parts = (got, dense_down, him, lom)
    shape = (nzx, seqs, slice_width)
    hold = [pltpu.VMEM((nzx, seqs, cols), f32)]
    sent = local(functools.partial(block_kernel, 1), "block_other", sds(shape), parts, hold)
    arrived = other_core(sent)
    kept = local(functools.partial(block_kernel, 0), "block_mine", sds(shape, f32), parts, hold)
    block = local(add_kernel, "add", sds(shape), (kept, arrived))
    got = exchange(block, ZX)
    out = local(final_kernel, "final", sds((seqs, slice_width)), (got, resid), keep=False)
    return out, new_keys, new_values


def solution(mesh):
    shape = (mesh.shape["ep"] // (2 * NX), NX, 2, mesh.shape["tp"])
    split = Mesh(mesh.devices.reshape(shape), ("z", "x", "c", "tp"))
    return jax.shard_map(
        body,
        mesh=split,
        in_specs=(
            P(EP, None),
            P(),
            P(EP, "tp"),
            P(EP, "tp"),
            P(EP, "tp"),
            P("tp"),
            P(EP, "tp", None, None),
            P(EP, "tp", None, None),
            P(EP),
            P("tp", EP),
            P(),
            P(),
            P("tp", EP),
            P("tp", EP),
            P(EP, "tp"),
            P(EP, None),
            P(EP, None),
            P(EP, None, "tp"),
            P(EP, None, "tp"),
            P(EP, "tp", None),
        ),
        out_specs=(P(EP, "tp"), P(EP, "tp"), P(EP, "tp")),
        check_vma=False,
    )
```

```python
import functools
import jax
import jax.numpy as jnp
from jax import lax
from jax.experimental import pallas as pl
from jax.experimental.pallas import tpu as pltpu
from jax.sharding import Mesh
from jax.sharding import PartitionSpec as P

EP = ("z", "x", "c")
ZX = ("z", "x")

norm_eps = 1e-05
clamp_limit = 7.0
swish_alpha = 1.702
f32 = jnp.float32
bf16 = jnp.bfloat16
VM = pl.BlockSpec(memory_space=pltpu.VMEM)
SM = pl.BlockSpec(memory_space=pltpu.SMEM)

NX = 4


def rms_scale(values, gain):
    return values * lax.rsqrt(jnp.mean(values * values, axis=-1, keepdims=True) + norm_eps) * gain


def clamped_unit(gate_pre, up_pre):
    gate_c = jnp.minimum(gate_pre, clamp_limit)
    up_c = jnp.clip(up_pre, -clamp_limit, clamp_limit)
    return (up_c + 1.0) * gate_c * jax.nn.sigmoid(swish_alpha * gate_c)


def exchange(blocks, axes):
    return lax.all_to_all(blocks, axes, 0, 0, tiled=True)


def other_core(values):
    return lax.ppermute(values, "c", [(0, 1), (1, 0)])


def along_x(values, k):
    return lax.ppermute(values, "x", [(i, (i + k) % NX) for i in range(NX)])


def local(kernel, name, outs, args, scratch=(), smem=0, keep=True, pin=pltpu.VMEM):
    multi = isinstance(outs, (list, tuple))
    if keep:
        outs = jax.tree.map(lambda s: pltpu.VMEM(s.shape, s.dtype), outs)
    pins = pin if isinstance(pin, tuple) else (pin,) * (len(args) - smem)
    args = tuple(args[:smem]) + tuple(
        pltpu.with_memory_space_constraint(a, p) for a, p in zip(args[smem:], pins)
    )
    return pl.pallas_call(
        kernel,
        out_shape=outs,
        in_specs=[SM] * smem + [VM] * (len(args) - smem),
        out_specs=[VM] * len(outs) if multi else VM,
        scratch_shapes=list(scratch),
        compiler_params=pltpu.CompilerParams(vmem_limit_bytes=16 << 20),
        name=name,
    )(*args)


def sds(shape, dtype=bf16):
    return jax.ShapeDtypeStruct(tuple(shape), dtype)


def pick(parts, at):
    out = parts[0]
    for k in range(1, len(parts)):
        out = jnp.where(at == k, parts[k], out)
    return out


def prepare_kernel(nz, tok, gain, qw, kw, vw, owt, ids, rw, wcat, msg):
    qc, kc = qw.shape[1], kw.shape[1]
    proj = qc + 2 * kc
    wcat[:, :qc] = qw[...]
    wcat[:, qc : qc + kc] = kw[...]
    wcat[:, qc + kc : proj] = vw[...]
    normed = rms_scale(tok[...].astype(f32), gain[...]).astype(bf16)
    seqs = normed.shape[0]
    lane = lax.broadcasted_iota(jnp.int32, (seqs, 128), 1)
    row = lax.broadcasted_iota(jnp.int32, (seqs, seqs), 0)
    col = lax.broadcasted_iota(jnp.int32, (seqs, seqs), 1)
    hi = rw[...].astype(bf16).astype(f32)
    lo = rw[...] - hi
    idf = ids[...].astype(f32)
    top = idf.shape[0]
    meta = jnp.zeros((seqs, 128), f32)
    for j, values in enumerate((idf, hi, lo)):
        for k in range(top):
            down = jnp.sum(jnp.where(row == col, values[k : k + 1], 0.0), axis=1, keepdims=True)
            meta = jnp.where(lane == j * top + k, down, meta)
    meta = meta.astype(bf16)
    wcat[:seqs, proj:] = meta
    wcat[seqs:, proj:] = jnp.zeros((wcat.shape[0] - seqs, 128), bf16)
    heads = owt.shape[1]
    for z in range(nz):
        msg[z, :, :heads] = owt[...]
        msg[z, :seqs, heads:] = normed[:, z * 256 : z * 256 + 128]
        msg[z, seqs:, heads:] = normed[:, z * 256 + 128 : z * 256 + 256]


def project_kernel(at, got, w0, w1, w2, w3, wo, part, owm, w_s, f_s):
    x, c = at[1], at[2]
    nz, depth, wide = got.shape
    seqs = depth // 2
    proj = w_s.shape[1]
    table = jnp.zeros((seqs, 128), f32)
    for k, w in enumerate((w0, w1, w2, w3)):
        place = lax.rem(x + NX - k, NX) * 2
        w_s[pl.ds(pl.multiple_of((place + c) * depth, depth), depth)] = w[:, :proj]
        w_s[pl.ds(pl.multiple_of((place + 1 - c) * depth, depth), depth)] = wo[k, :, :proj]
        table += pltpu.roll(w[:seqs, proj:].astype(f32), k * 16, 1)
        table += pltpu.roll(wo[k, :seqs, proj:].astype(f32), (NX + k) * 16, 1)
    table = table.astype(bf16)
    for z in range(nz):
        f_s[z * seqs : (z + 1) * seqs, :128] = got[z, :seqs, wide - 128 :]
        f_s[z * seqs : (z + 1) * seqs, 128:] = got[z, seqs:, wide - 128 :]
        owm[z] = got[z, :, : wide - 128]
    out = jnp.dot(f_s[...], w_s[...], preferred_element_type=f32).astype(bf16)
    for z in range(nz):
        part[z, :, :proj] = out[z * seqs : (z + 1) * seqs]
        part[z, :, proj:] = table


def attention_kernel(
    block, lengths, bias, part, k_hbm, v_hbm, att, nk, nv, k_ref, v_ref, q_s, z_s, w_s, sems
):
    seqs, _, span, head_dim = k_ref.shape
    piece = 256
    steps = span // piece
    pairs = ((k_hbm, k_ref), (v_hbm, v_ref))

    def each_size(which, s, act):
        live = lax.div(lengths[s] + piece - 1, piece)
        for n in range(1, steps + 1):

            @pl.when(live == n)
            def _():
                place = (s, 0, pl.ds(0, n * piece))
                source, target = pairs[which]
                act(
                    pltpu.make_async_copy(source.at[place], target.at[place], sems.at[which, s]), n
                )

    def begin(copy, n):
        copy.start()

    @pl.loop(0, seqs)
    def _(s):
        each_size(0, s, begin)

    @pl.loop(0, seqs)
    def _(s):
        def clear(copy, n):
            copy.start()
            if n < steps:
                rest = (steps - n) * piece
                v_ref[s, 0, pl.ds(n * piece, rest)] = jnp.zeros((rest, head_dim), bf16)

        each_size(1, s, clear)

    heads = bias.shape[0]
    q_cols = heads * head_dim
    both = 2 * heads
    qkv = jnp.sum(part[:, :, : q_cols + 2 * head_dim].astype(f32), axis=0)
    nk[...] = qkv[:, q_cols : q_cols + head_dim].astype(bf16)
    nv[...] = qkv[:, q_cols + head_dim :].astype(bf16)
    for s in range(seqs):
        for h in range(heads):
            at_row = s * heads + h
            q_s[at_row : at_row + 1] = qkv[s : s + 1, h * head_dim : (h + 1) * head_dim]

    upper = lax.broadcasted_iota(jnp.int32, (both, 1), 0) < heads

    def wait(copy, n):
        copy.wait()

    @pl.loop(0, seqs // 2)
    def _(i):
        s = i * 2
        each_size(0, s, wait)
        each_size(0, s + 1, wait)
        here = pl.ds(pl.multiple_of(s * heads, both), both)
        q = q_s[here].astype(bf16)
        pair = [
            lax.dot_general(
                q, k_ref[s + j, 0], (((1,), (1,)), ((), ())), preferred_element_type=f32
            )
            for j in range(2)
        ]
        z_s[here] = jnp.where(upper, pair[0], pair[1])

    rows = block * heads
    row = lax.broadcasted_iota(jnp.int32, (rows, 1), 0)
    lane = lax.broadcasted_iota(jnp.int32, (rows, 128), 1)
    offset = jnp.zeros((rows, 1), f32)
    for h in range(heads):
        offset = jnp.where(row % heads == h, bias[h], offset)
    chunks = span // 128

    @pl.loop(0, seqs // block)
    def _(step):
        length = jnp.zeros((rows, 1), jnp.int32)
        for i in range(block):
            length = jnp.where(row // heads == i, lengths[step * block + i], length)
        here = pl.ds(pl.multiple_of(step * rows, rows), rows)
        after = jnp.zeros((rows, 1), f32)
        for c in range(chunks - 1, -1, -1):
            cols = slice(c * 128, (c + 1) * 128)
            z = z_s[here, cols] * head_dim ** (-0.5) + offset
            inside = lane + c * 128 < length
            tail = jnp.log1p(jnp.exp(-jnp.abs(z)))
            keep = jnp.where(inside, -jnp.maximum(z, 0.0) - tail, 0.0)
            total = keep
            shift = 1
            while shift < 128:
                moved = pltpu.roll(total, 128 - shift, 1)
                total = total + jnp.where(lane < 128 - shift, moved, 0.0)
                shift *= 2
            between = total - keep + after
            after = after + total[:, 0:1]
            power = jnp.exp(jnp.minimum(z, 0.0) - tail + between)
            w_s[here, cols] = jnp.where(inside, power, 0.0)

    @pl.loop(0, seqs // 2)
    def _(i):
        s = i * 2
        each_size(1, s, wait)
        each_size(1, s + 1, wait)
        here = pl.ds(pl.multiple_of(s * heads, both), both)
        w = w_s[here].astype(bf16)
        pair = [jnp.dot(w, v_ref[s + j, 0], preferred_element_type=f32) for j in range(2)]
        q_s[here] = jnp.where(upper, pair[0], pair[1])

    out = q_s[...].astype(bf16).astype(f32)
    for s in range(seqs):
        for h in range(heads):
            at_row = s * heads + h
            att[s : s + 1, h * head_dim : (h + 1) * head_dim] = out[at_row : at_row + 1].astype(
                bf16
            )


def attention(part, bias, keys, values, lengths):
    seqs, _, span, head_dim = keys.shape
    heads = bias.shape[0]
    outs = [sds((seqs, heads * head_dim)), sds((seqs, head_dim)), sds((seqs, head_dim))]
    hbm = pl.BlockSpec(memory_space=pltpu.HBM)
    pins = (pltpu.VMEM, pltpu.HBM, pltpu.HBM)
    args = [
        pltpu.with_memory_space_constraint(a, p) for a, p in zip((part, keys, values), pins)
    ]
    return pl.pallas_call(
        functools.partial(attention_kernel, 8),
        out_shape=outs,
        in_specs=[SM, SM, VM, hbm, hbm],
        out_specs=[VM] * 3,
        scratch_shapes=[pltpu.VMEM(keys.shape, bf16)] * 2
        + [pltpu.VMEM((seqs * heads, head_dim), f32)]
        + [pltpu.VMEM((seqs * heads, span), f32)] * 2
        + [pltpu.SemaphoreType.DMA((2, seqs))],
        compiler_params=pltpu.CompilerParams(vmem_limit_bytes=24 << 20),
        name="attention",
    )(*(pltpu.with_memory_space_constraint(a, pltpu.HBM) for a in (lengths, bias)), *args)


def mix_kernel(at, att, *refs):
    mine, others, msg, w_s = refs[:NX], refs[NX : 2 * NX], refs[2 * NX], refs[2 * NX + 1]
    x, c = at[1], at[2]
    nz, depth = mine[0].shape[:2]
    heads = att.shape[1]
    for k in range(NX):
        place = lax.rem(x + NX - k, NX) * 2
        for z in range(nz):
            base = z * NX * 2
            w_s[pl.ds(pl.multiple_of((base + place + c) * depth, depth), depth)] = mine[k][
                z, :, :heads
            ]
            w_s[pl.ds(pl.multiple_of((base + place + 1 - c) * depth, depth), depth)] = others[k][
                z, :, :heads
            ]
    out = lax.dot_general(
        att[...], w_s[...], (((1,), (1,)), ((), ())), preferred_element_type=f32
    ).astype(bf16)
    for t in range(msg.shape[0]):
        msg[t] = out


def slots_kernel(seqs, top, at, part, him, lom, m_s):
    x = at[1]
    nz, _, wide = part.shape
    for z in range(nz):
        table = part[z, :, wide - 128 :].astype(f32)
        for k in range(NX):
            place = lax.rem(x + NX - k, NX) * seqs
            start = pl.multiple_of(z * NX * seqs + place, seqs)
            m_s[pl.ds(start, seqs)] = pltpu.roll(table, (128 - k * 16) % 128, 1)
    m = m_s[...]
    rows = m.shape[0]
    lane = lax.broadcasted_iota(jnp.int32, (rows, 128), 1)
    row = lax.broadcasted_iota(jnp.int32, (rows, 128), 0)
    highs = pltpu.roll(m, 128 - top, 1)
    lows = pltpu.roll(m, 128 - 2 * top, 1)
    him_all = jnp.zeros((rows, 128), f32)
    lom_all = jnp.zeros((rows, 128), f32)
    for c in range(2):
        expert = (at[0] * NX + x) * 2 + c
        hit = jnp.where((m == expert.astype(f32)) & (lane < top), 1.0, 0.0)
        hi = jnp.sum(hit * highs, axis=1, keepdims=True)
        lo = jnp.sum(hit * lows, axis=1, keepdims=True)
        own = jnp.broadcast_to(jnp.sum(hit, axis=1, keepdims=True), (rows, 128))
        upto = own
        shift = 1
        while shift < seqs:
            upto = upto + jnp.where(row % seqs >= shift, pltpu.roll(upto, shift, 0), 0.0)
            shift *= 2
        slot = c * 64 + (row // seqs) * 2 + (upto - own).astype(jnp.int32)
        here = jnp.where((lane == slot) & (own > 0.5), 1.0, 0.0)
        him_all += here * hi
        lom_all += here * lo
    him[...] = him_all.astype(bf16)
    lom[...] = lom_all.astype(bf16)


def norm_kernel(at, got, tok, gain, ids, msg, res):
    t = at[3]
    mixed = jnp.sum(got[...].astype(f32), axis=0).astype(bf16).astype(f32)
    resid = tok[...].astype(f32) + mixed
    normed = rms_scale(resid, gain[...]).astype(bf16)
    seqs, width = resid.shape
    nb, share, _ = msg.shape
    parts = got.shape[0]
    wide = width // parts
    own = share // 2
    res[...] = pick([resid[:, k * wide : (k + 1) * wide] for k in range(parts)], t)
    top = ids.shape[0]
    experts = 2 * nb
    expert = lax.broadcasted_iota(jnp.int32, (experts, seqs), 0)
    hit = jnp.zeros((experts, seqs), f32)
    for k in range(top):
        hit = jnp.where(ids[k : k + 1] == expert, 1.0, hit)
    lane = lax.broadcasted_iota(jnp.int32, (seqs, seqs), 1)
    before = jnp.where(lax.broadcasted_iota(jnp.int32, (seqs, seqs), 0) < lane, 1.0, 0.0)
    rank = jnp.dot(hit, before, preferred_element_type=f32)
    quarter = lax.broadcasted_iota(jnp.int32, (own, seqs), 0) + t * own
    quarter = jnp.where(quarter == lax.broadcasted_iota(jnp.int32, (own, seqs), 1), 1.0, 0.0)
    first = jnp.where(rank < 0.5, hit, 0.0)
    second = jnp.where(rank > 0.5, hit, 0.0)
    choose = []
    for b in range(nb):
        choose.append(quarter)
        for c in range(2):
            e = 2 * b + c
            choose.append(first[e : e + 1])
            choose.append(second[e : e + 1])
    choose = jnp.concatenate(choose, axis=0).astype(bf16)
    rows = jnp.dot(choose, normed, preferred_element_type=f32).astype(bf16)
    msg[...] = rows.reshape(msg.shape)


def expert_kernel(
    at, mine, other, w0, w1, w2, w3, bg, eg, eu, ed, msg, w_s, d_s, x_s, r_s, sems
):
    t = at[3]
    nb, share, width = mine.shape
    own = share // 2
    nt = msg.shape[0] // 2
    slots = 2 * msg.shape[1]
    wide = width // nt
    cols = w0.shape[1] // 2
    copies = [pltpu.make_async_copy(ed.at[0], d_s, sems.at[nt])]
    for k, w in enumerate((w0, w1, w2, w3)):
        place = pl.multiple_of(lax.rem(t + nt - k, nt) * wide, wide)
        copies.append(pltpu.make_async_copy(w, w_s.at[pl.ds(place, wide)], sems.at[k]))
    for copy in copies:
        copy.start()
    core = at[2]
    half = nb * own
    for h, part in enumerate((mine, other)):
        block = part[...].astype(f32)
        routed = jnp.where(core == 0, block[:, own : own + 2], block[:, own + 2 :])
        r_s[h * 2 * nb : (h + 1) * 2 * nb] = routed.reshape(2 * nb, width).astype(bf16)
        x_s[h * half : (h + 1) * half] = block[:, :own].reshape(half, width).astype(bf16)
    rows = r_s[...]
    gate_pre = jnp.dot(rows, eg[0], preferred_element_type=f32)
    up_pre = jnp.dot(rows, eu[0], preferred_element_type=f32)
    act = clamped_unit(gate_pre, up_pre).astype(bf16)
    copies[0].wait()
    out = jnp.dot(act, d_s[...], preferred_element_type=f32).astype(bf16)
    some = slots // 2
    for r in range(2):
        to = lax.rem(core + r, 2) * nt
        for q in range(nt):
            msg[to + q, :, :wide] = out[r * some : (r + 1) * some, q * wide : (q + 1) * wide]
    x = x_s[...]
    gate = jnp.broadcast_to(bg[...].astype(f32), (8, width)).astype(bf16)
    branch = lax.dot_general(x, gate, (((1,), (1,)), ((), ())), preferred_element_type=f32)
    for copy in copies[1:]:
        copy.wait()
    pre = jnp.dot(x, w_s[...], preferred_element_type=f32)
    hidden = jax.nn.silu(pre[:, :cols]) * pre[:, cols:] * jax.nn.sigmoid(branch[:, 0:1])
    hidden = hidden.astype(bf16)
    for r in range(2):
        to = lax.rem(core + r, 2) * nt
        for q in range(nt):
            msg[to + q, :, wide : wide + cols] = hidden[r * half : r * half + some]
            msg[to + q, :, wide + cols :] = hidden[r * half + some : (r + 1) * half]


def block_kernel(at, got, dd, dd_other, him, lom, out, h_s):
    nt = got.shape[0] // 2
    some = got.shape[1]
    cols = dd.shape[0]
    wide = dd.shape[1]
    nb, seqs, _ = out.shape
    own = seqs // nt
    rows = []
    for c in range(2):
        part = jnp.sum(got[c * nt : (c + 1) * nt, :, :wide].astype(f32), axis=0)
        rows.append(part.astype(bf16))
        for q in range(nt):
            for f in range(2):
                start = wide + f * cols
                part = got[c * nt + q, :, start : start + cols].astype(f32)
                h_s[
                    f * nb // 2 : (f + 1) * nb // 2,
                    q * own : (q + 1) * own,
                    c * cols : (c + 1) * cols,
                ] = part.reshape(nb // 2, own, cols)
    hidden = h_s[...].reshape(nb * seqs, 2 * cols).astype(bf16)
    left = jnp.concatenate([hidden, him[...], lom[...]], axis=1)
    zero = at[2] == 0
    right = jnp.concatenate(
        [
            jnp.where(zero, dd[...], dd_other[...]),
            jnp.where(zero, dd_other[...], dd[...]),
            *rows,
            *rows,
        ],
        axis=0,
    )
    full = jnp.dot(left, right, preferred_element_type=f32)
    out[...] = full.astype(bf16).reshape(out.shape)


def final_kernel(got, res, out):
    out[...] = (jnp.sum(got[...].astype(f32), axis=0) + res[...]).astype(bf16)


def body(
    tokens,
    attn_gain,
    query_weight,
    key_weight,
    value_weight,
    break_bias,
    cache_keys,
    cache_values,
    lengths,
    out_weight,
    ffn_gain,
    branch_gate,
    dense_gate,
    dense_up,
    dense_down,
    route_ids,
    route_weights,
    expert_gate,
    expert_up,
    expert_down,
):
    nz, nt = lax.axis_size("z"), lax.axis_size("tp")
    nzx = nz * NX
    seqs, width = tokens.shape
    top = route_ids.shape[1]
    slice_width = width // nt
    all_rows = 2 * nzx * seqs
    slots = 2 * nzx * 2
    depth = query_weight.shape[0]
    heads = out_weight.shape[0]
    proj = query_weight.shape[1] + 2 * key_weight.shape[1]
    at = jnp.stack([lax.axis_index(a) for a in ("z", "x", "c", "tp")]).astype(jnp.int32)

    wcat, msg = local(
        functools.partial(prepare_kernel, nz),
        "prepare",
        [sds((depth, proj + 128)), sds((nz, depth, heads + 128))],
        (
            tokens,
            attn_gain[None],
            query_weight,
            key_weight,
            value_weight,
            out_weight.T,
            route_ids.T,
            route_weights.T,
        ),
        pin=pltpu.HBM,
    )
    with jax.named_scope("over_z"):
        got = exchange(msg, "z")
    with jax.named_scope("weights_x"):
        w_x = [wcat] + [along_x(wcat, k) for k in range(1, NX)]
    w_other = other_core(jnp.stack(w_x))
    part, owm = local(
        project_kernel,
        "project",
        [sds((nz, seqs, proj + 128)), sds((nz, depth, heads))],
        (at, got, *w_x, w_other),
        [pltpu.VMEM((2 * NX * depth, proj), bf16), pltpu.VMEM((nz * seqs, 2 * NX * depth), bf16)],
        smem=1,
    )
    with jax.named_scope("partial_z"):
        part = exchange(part, "z")
    with jax.named_scope("mix_x"):
        ow = [owm] + [along_x(owm, k) for k in range(1, NX)]
    ow_other = [other_core(piece) for piece in ow]

    attended, new_keys, new_values = attention(
        part, break_bias, cache_keys, cache_values, lengths
    )

    msg = local(
        mix_kernel,
        "mix",
        sds((nt, seqs, width)),
        (at, attended, *ow, *ow_other),
        [pltpu.VMEM((width, heads), bf16)],
        smem=1,
    )
    mixed = exchange(msg, "tp")
    him, lom = local(
        functools.partial(slots_kernel, seqs, top),
        "slots",
        [sds((all_rows // 2, slots))] * 2,
        (at, part),
        [pltpu.VMEM((all_rows // 2, 128), f32)],
        smem=1,
    )
    own = seqs // nt
    cols = dense_gate.shape[1]
    msg, resid = local(
        norm_kernel,
        "norm",
        [sds((nzx, 2 * own, width)), sds((seqs, slice_width), f32)],
        (at, mixed, tokens, ffn_gain[None], route_ids.T),
        smem=1,
    )
    with jax.named_scope("rows_zx"):
        mine = exchange(msg, ZX)
    with jax.named_scope("dense_tp"):
        gu = jnp.concatenate([dense_gate, dense_up], axis=1)
        gu = [gu] + [
            lax.ppermute(gu, "tp", [(i, (i + k) % nt) for i in range(nt)]) for k in range(1, nt)
        ]
        down = other_core(dense_down)
    mine, down, *gu = lax.optimization_barrier((mine, down, *gu))
    other, him, lom = lax.optimization_barrier((other_core(mine), him, lom))
    hbm = pl.BlockSpec(memory_space=pltpu.HBM)
    places = [pltpu.VMEM] * 2 + [pltpu.HBM] * nt + [pltpu.VMEM] * 3 + [pltpu.HBM]
    operands = (mine, other, *gu, branch_gate[None], expert_gate, expert_up, expert_down)
    msg = pl.pallas_call(
        expert_kernel,
        out_shape=pltpu.VMEM((2 * nt, slots // 2, slice_width + 2 * cols), bf16),
        in_specs=[SM] + [hbm if p == pltpu.HBM else VM for p in places],
        out_specs=VM,
        scratch_shapes=[
            pltpu.VMEM((width, 2 * cols), bf16),
            pltpu.VMEM(expert_down.shape[1:], bf16),
            pltpu.VMEM((2 * nzx * own, width), bf16),
            pltpu.VMEM((slots, width), bf16),
            pltpu.SemaphoreType.DMA((nt + 1,)),
        ],
        compiler_params=pltpu.CompilerParams(vmem_limit_bytes=16 << 20),
        name="expert",
    )(at, *(pltpu.with_memory_space_constraint(a, p) for a, p in zip(operands, places)))
    got = exchange(msg, ("c", "tp"))
    block = local(
        block_kernel,
        "block",
        sds((nzx, seqs, slice_width)),
        (at, got, dense_down, down, him, lom),
        [pltpu.VMEM((nzx, seqs, 2 * cols), f32)],
        smem=1,
    )
    got = exchange(block, ZX)
    out = local(final_kernel, "final", sds((seqs, slice_width)), (got, resid), keep=False)
    return out, new_keys, new_values


def solution(mesh):
    shape = (mesh.shape["ep"] // (2 * NX), NX, 2, mesh.shape["tp"])
    split = Mesh(mesh.devices.reshape(shape), ("z", "x", "c", "tp"))
    return jax.shard_map(
        body,
        mesh=split,
        in_specs=(
            P(EP, None),
            P(),
            P(EP, "tp"),
            P(EP, "tp"),
            P(EP, "tp"),
            P("tp"),
            P(EP, "tp", None, None),
            P(EP, "tp", None, None),
            P(EP),
            P("tp", EP),
            P(),
            P(),
            P("tp", EP),
            P("tp", EP),
            P(EP, "tp"),
            P(EP, None),
            P(EP, None),
            P(EP, None, "tp"),
            P(EP, None, "tp"),
            P(EP, "tp", None),
        ),
        out_specs=(P(EP, "tp"), P(EP, "tp"), P(EP, "tp")),
        check_vma=False,
    )
```

```python
import functools
import jax
import jax.numpy as jnp
from jax import lax
from jax.experimental import pallas as pl
from jax.experimental.pallas import tpu as pltpu
from jax.sharding import Mesh
from jax.sharding import PartitionSpec as P

EP = ("z", "x", "c")
ZX = ("z", "x")

norm_eps = 1e-05
clamp_limit = 7.0
swish_alpha = 1.702
f32 = jnp.float32
bf16 = jnp.bfloat16
VM = pl.BlockSpec(memory_space=pltpu.VMEM)
SM = pl.BlockSpec(memory_space=pltpu.SMEM)

NX = 4


def rms_scale(values, gain):
    return values * lax.rsqrt(jnp.mean(values * values, axis=-1, keepdims=True) + norm_eps) * gain


def clamped_unit(gate_pre, up_pre):
    gate_c = jnp.minimum(gate_pre, clamp_limit)
    up_c = jnp.clip(up_pre, -clamp_limit, clamp_limit)
    return (up_c + 1.0) * gate_c * jax.nn.sigmoid(swish_alpha * gate_c)


def exchange(blocks, axes):
    return lax.all_to_all(blocks, axes, 0, 0, tiled=True)


def other_core(values):
    return lax.ppermute(values, "c", [(0, 1), (1, 0)])


def along_x(values, k):
    return lax.ppermute(values, "x", [(i, (i + k) % NX) for i in range(NX)])


def local(kernel, name, outs, args, scratch=(), smem=0, keep=True, pin=pltpu.VMEM):
    multi = isinstance(outs, (list, tuple))
    if keep:
        outs = jax.tree.map(lambda s: pltpu.VMEM(s.shape, s.dtype), outs)
    pins = pin if isinstance(pin, tuple) else (pin,) * (len(args) - smem)
    args = tuple(args[:smem]) + tuple(
        pltpu.with_memory_space_constraint(a, p) for a, p in zip(args[smem:], pins)
    )
    return pl.pallas_call(
        kernel,
        out_shape=outs,
        in_specs=[SM] * smem + [VM] * (len(args) - smem),
        out_specs=[VM] * len(outs) if multi else VM,
        scratch_shapes=list(scratch),
        compiler_params=pltpu.CompilerParams(vmem_limit_bytes=16 << 20),
        name=name,
    )(*args)


def sds(shape, dtype=bf16):
    return jax.ShapeDtypeStruct(tuple(shape), dtype)


def pick(parts, at):
    out = parts[0]
    for k in range(1, len(parts)):
        out = jnp.where(at == k, parts[k], out)
    return out


def prepare_kernel(nz, tok, gain, qw, kw, vw, owt, ids, rw, wcat, msg):
    qc, kc = qw.shape[1], kw.shape[1]
    proj = qc + 2 * kc
    wcat[:, :qc] = qw[...]
    wcat[:, qc : qc + kc] = kw[...]
    wcat[:, qc + kc : proj] = vw[...]
    normed = rms_scale(tok[...].astype(f32), gain[...]).astype(bf16)
    seqs = normed.shape[0]
    lane = lax.broadcasted_iota(jnp.int32, (seqs, 128), 1)
    row = lax.broadcasted_iota(jnp.int32, (seqs, seqs), 0)
    col = lax.broadcasted_iota(jnp.int32, (seqs, seqs), 1)
    hi = rw[...].astype(bf16).astype(f32)
    lo = rw[...] - hi
    idf = ids[...].astype(f32)
    top = idf.shape[0]
    meta = jnp.zeros((seqs, 128), f32)
    for j, values in enumerate((idf, hi, lo)):
        for k in range(top):
            down = jnp.sum(jnp.where(row == col, values[k : k + 1], 0.0), axis=1, keepdims=True)
            meta = jnp.where(lane == j * top + k, down, meta)
    meta = meta.astype(bf16)
    wcat[:seqs, proj:] = meta
    wcat[seqs:, proj:] = jnp.zeros((wcat.shape[0] - seqs, 128), bf16)
    heads = owt.shape[1]
    for z in range(nz):
        msg[z, :, :heads] = owt[...]
        msg[z, :seqs, heads:] = normed[:, z * 256 : z * 256 + 128]
        msg[z, seqs:, heads:] = normed[:, z * 256 + 128 : z * 256 + 256]


def project_kernel(at, got, w0, w1, w2, w3, wo, part, owm, w_s, f_s):
    x, c = at[1], at[2]
    nz, depth, wide = got.shape
    seqs = depth // 2
    proj = w_s.shape[1]
    table = jnp.zeros((seqs, 128), f32)
    for k, w in enumerate((w0, w1, w2, w3)):
        place = lax.rem(x + NX - k, NX) * 2
        w_s[pl.ds(pl.multiple_of((place + c) * depth, depth), depth)] = w[:, :proj]
        w_s[pl.ds(pl.multiple_of((place + 1 - c) * depth, depth), depth)] = wo[k, :, :proj]
        table += pltpu.roll(w[:seqs, proj:].astype(f32), k * 16, 1)
        table += pltpu.roll(wo[k, :seqs, proj:].astype(f32), (NX + k) * 16, 1)
    table = table.astype(bf16)
    for z in range(nz):
        f_s[z * seqs : (z + 1) * seqs, :128] = got[z, :seqs, wide - 128 :]
        f_s[z * seqs : (z + 1) * seqs, 128:] = got[z, seqs:, wide - 128 :]
        owm[z] = got[z, :, : wide - 128]
    out = jnp.dot(f_s[...], w_s[...], preferred_element_type=f32).astype(bf16)
    for z in range(nz):
        part[z, :, :proj] = out[z * seqs : (z + 1) * seqs]
        part[z, :, proj:] = table


def attention_kernel(
    block, lengths, bias, part, k_hbm, v_hbm, att, nk, nv, k_ref, v_ref, q_s, z_s, w_s, sems
):
    seqs, _, span, head_dim = k_ref.shape
    piece = 256
    steps = span // piece
    pairs = ((k_hbm, k_ref), (v_hbm, v_ref))

    def each_size(which, s, act):
        live = lax.div(lengths[s] + piece - 1, piece)
        for n in range(1, steps + 1):

            @pl.when(live == n)
            def _():
                place = (s, 0, pl.ds(0, n * piece))
                source, target = pairs[which]
                act(
                    pltpu.make_async_copy(source.at[place], target.at[place], sems.at[which, s]), n
                )

    def begin(copy, n):
        copy.start()

    @pl.loop(0, seqs)
    def _(s):
        each_size(0, s, begin)

    @pl.loop(0, seqs)
    def _(s):
        def clear(copy, n):
            copy.start()
            if n < steps:
                rest = (steps - n) * piece
                v_ref[s, 0, pl.ds(n * piece, rest)] = jnp.zeros((rest, head_dim), bf16)

        each_size(1, s, clear)

    heads = bias.shape[0]
    q_cols = heads * head_dim
    both = 2 * heads
    qkv = jnp.sum(part[:, :, : q_cols + 2 * head_dim].astype(f32), axis=0)
    nk[...] = qkv[:, q_cols : q_cols + head_dim].astype(bf16)
    nv[...] = qkv[:, q_cols + head_dim :].astype(bf16)
    for s in range(seqs):
        for h in range(heads):
            at_row = s * heads + h
            q_s[at_row : at_row + 1] = qkv[s : s + 1, h * head_dim : (h + 1) * head_dim]

    upper = lax.broadcasted_iota(jnp.int32, (both, 1), 0) < heads

    def wait(copy, n):
        copy.wait()

    @pl.loop(0, seqs // 2, unroll=4)
    def _(i):
        s = i * 2
        each_size(0, s, wait)
        each_size(0, s + 1, wait)
        here = pl.ds(pl.multiple_of(s * heads, both), both)
        q = q_s[here].astype(bf16)
        pair = [
            lax.dot_general(
                q, k_ref[s + j, 0], (((1,), (1,)), ((), ())), preferred_element_type=f32
            )
            for j in range(2)
        ]
        z_s[here] = jnp.where(upper, pair[0], pair[1])

    rows = block * heads
    row = lax.broadcasted_iota(jnp.int32, (rows, 1), 0)
    lane = lax.broadcasted_iota(jnp.int32, (rows, 128), 1)
    offset = jnp.zeros((rows, 1), f32)
    for h in range(heads):
        offset = jnp.where(row % heads == h, bias[h], offset)
    chunks = span // 128

    @pl.loop(0, seqs // block)
    def _(step):
        length = jnp.zeros((rows, 1), jnp.int32)
        for i in range(block):
            length = jnp.where(row // heads == i, lengths[step * block + i], length)
        here = pl.ds(pl.multiple_of(step * rows, rows), rows)
        after = jnp.zeros((rows, 1), f32)
        for c in range(chunks - 1, -1, -1):
            cols = slice(c * 128, (c + 1) * 128)
            z = z_s[here, cols] * head_dim ** (-0.5) + offset
            inside = lane + c * 128 < length
            tail = jnp.log1p(jnp.exp(-jnp.abs(z)))
            keep = jnp.where(inside, -jnp.maximum(z, 0.0) - tail, 0.0)
            total = keep
            shift = 1
            while shift < 128:
                moved = pltpu.roll(total, 128 - shift, 1)
                total = total + jnp.where(lane < 128 - shift, moved, 0.0)
                shift *= 2
            between = total - keep + after
            after = after + total[:, 0:1]
            power = jnp.exp(jnp.minimum(z, 0.0) - tail + between)
            w_s[here, cols] = jnp.where(inside, power, 0.0)

    @pl.loop(0, seqs // 2, unroll=4)
    def _(i):
        s = i * 2
        each_size(1, s, wait)
        each_size(1, s + 1, wait)
        here = pl.ds(pl.multiple_of(s * heads, both), both)
        w = w_s[here].astype(bf16)
        pair = [jnp.dot(w, v_ref[s + j, 0], preferred_element_type=f32) for j in range(2)]
        q_s[here] = jnp.where(upper, pair[0], pair[1])

    out = q_s[...].astype(bf16).astype(f32)
    for s in range(seqs):
        for h in range(heads):
            at_row = s * heads + h
            att[s : s + 1, h * head_dim : (h + 1) * head_dim] = out[at_row : at_row + 1].astype(
                bf16
            )


def attention(part, bias, keys, values, lengths):
    seqs, _, span, head_dim = keys.shape
    heads = bias.shape[0]
    outs = [sds((seqs, heads * head_dim)), sds((seqs, head_dim)), sds((seqs, head_dim))]
    hbm = pl.BlockSpec(memory_space=pltpu.HBM)
    pins = (pltpu.VMEM, pltpu.HBM, pltpu.HBM)
    args = [
        pltpu.with_memory_space_constraint(a, p) for a, p in zip((part, keys, values), pins)
    ]
    return pl.pallas_call(
        functools.partial(attention_kernel, 16),
        out_shape=outs,
        in_specs=[SM, SM, VM, hbm, hbm],
        out_specs=[VM] * 3,
        scratch_shapes=[pltpu.VMEM(keys.shape, bf16)] * 2
        + [pltpu.VMEM((seqs * heads, head_dim), f32)]
        + [pltpu.VMEM((seqs * heads, span), f32)] * 2
        + [pltpu.SemaphoreType.DMA((2, seqs))],
        compiler_params=pltpu.CompilerParams(vmem_limit_bytes=24 << 20),
        name="attention",
    )(*(pltpu.with_memory_space_constraint(a, pltpu.HBM) for a in (lengths, bias)), *args)


def mix_kernel(at, att, *refs):
    mine, others, msg, w_s = refs[:NX], refs[NX : 2 * NX], refs[2 * NX], refs[2 * NX + 1]
    x, c = at[1], at[2]
    nz, depth = mine[0].shape[:2]
    heads = att.shape[1]
    for k in range(NX):
        place = lax.rem(x + NX - k, NX) * 2
        for z in range(nz):
            base = z * NX * 2
            w_s[pl.ds(pl.multiple_of((base + place + c) * depth, depth), depth)] = mine[k][
                z, :, :heads
            ]
            w_s[pl.ds(pl.multiple_of((base + place + 1 - c) * depth, depth), depth)] = others[k][
                z, :, :heads
            ]
    out = lax.dot_general(
        att[...], w_s[...], (((1,), (1,)), ((), ())), preferred_element_type=f32
    ).astype(bf16)
    for t in range(msg.shape[0]):
        msg[t] = out


def slots_kernel(seqs, top, at, part, him, lom, m_s):
    x = at[1]
    nz, _, wide = part.shape
    for z in range(nz):
        table = part[z, :, wide - 128 :].astype(f32)
        for k in range(NX):
            place = lax.rem(x + NX - k, NX) * seqs
            start = pl.multiple_of(z * NX * seqs + place, seqs)
            m_s[pl.ds(start, seqs)] = pltpu.roll(table, (128 - k * 16) % 128, 1)
    m = m_s[...]
    rows = m.shape[0]
    lane = lax.broadcasted_iota(jnp.int32, (rows, 128), 1)
    row = lax.broadcasted_iota(jnp.int32, (rows, 128), 0)
    highs = pltpu.roll(m, 128 - top, 1)
    lows = pltpu.roll(m, 128 - 2 * top, 1)
    him_all = jnp.zeros((rows, 128), f32)
    lom_all = jnp.zeros((rows, 128), f32)
    for c in range(2):
        expert = (at[0] * NX + x) * 2 + c
        hit = jnp.where((m == expert.astype(f32)) & (lane < top), 1.0, 0.0)
        hi = jnp.sum(hit * highs, axis=1, keepdims=True)
        lo = jnp.sum(hit * lows, axis=1, keepdims=True)
        own = jnp.broadcast_to(jnp.sum(hit, axis=1, keepdims=True), (rows, 128))
        upto = own
        shift = 1
        while shift < seqs:
            upto = upto + jnp.where(row % seqs >= shift, pltpu.roll(upto, shift, 0), 0.0)
            shift *= 2
        slot = c * 64 + (row // seqs) * 2 + (upto - own).astype(jnp.int32)
        here = jnp.where((lane == slot) & (own > 0.5), 1.0, 0.0)
        him_all += here * hi
        lom_all += here * lo
    him[...] = him_all.astype(bf16)
    lom[...] = lom_all.astype(bf16)


def norm_kernel(at, got, tok, gain, ids, msg, res):
    t = at[3]
    mixed = jnp.sum(got[...].astype(f32), axis=0).astype(bf16).astype(f32)
    resid = tok[...].astype(f32) + mixed
    normed = rms_scale(resid, gain[...]).astype(bf16)
    seqs, width = resid.shape
    nb, share, _ = msg.shape
    parts = got.shape[0]
    wide = width // parts
    own = share // 2
    res[...] = pick([resid[:, k * wide : (k + 1) * wide] for k in range(parts)], t)
    top = ids.shape[0]
    experts = 2 * nb
    expert = lax.broadcasted_iota(jnp.int32, (experts, seqs), 0)
    hit = jnp.zeros((experts, seqs), f32)
    for k in range(top):
        hit = jnp.where(ids[k : k + 1] == expert, 1.0, hit)
    lane = lax.broadcasted_iota(jnp.int32, (seqs, seqs), 1)
    before = jnp.where(lax.broadcasted_iota(jnp.int32, (seqs, seqs), 0) < lane, 1.0, 0.0)
    rank = jnp.dot(hit, before, preferred_element_type=f32)
    quarter = lax.broadcasted_iota(jnp.int32, (own, seqs), 0) + t * own
    quarter = jnp.where(quarter == lax.broadcasted_iota(jnp.int32, (own, seqs), 1), 1.0, 0.0)
    first = jnp.where(rank < 0.5, hit, 0.0)
    second = jnp.where(rank > 0.5, hit, 0.0)
    choose = []
    for b in range(nb):
        choose.append(quarter)
        for c in range(2):
            e = 2 * b + c
            choose.append(first[e : e + 1])
            choose.append(second[e : e + 1])
    choose = jnp.concatenate(choose, axis=0).astype(bf16)
    rows = jnp.dot(choose, normed, preferred_element_type=f32).astype(bf16)
    msg[...] = rows.reshape(msg.shape)


def expert_kernel(
    at, mine, other, w0, w1, w2, w3, bg, eg, eu, ed, msg, w_s, d_s, x_s, r_s, sems
):
    t = at[3]
    nb, share, width = mine.shape
    own = share // 2
    nt = msg.shape[0] // 2
    slots = 2 * msg.shape[1]
    wide = width // nt
    cols = w0.shape[1] // 2
    copies = [pltpu.make_async_copy(ed.at[0], d_s, sems.at[nt])]
    for k, w in enumerate((w0, w1, w2, w3)):
        place = pl.multiple_of(lax.rem(t + nt - k, nt) * wide, wide)
        copies.append(pltpu.make_async_copy(w, w_s.at[pl.ds(place, wide)], sems.at[k]))
    for copy in copies:
        copy.start()
    core = at[2]
    half = nb * own
    for h, part in enumerate((mine, other)):
        block = part[...].astype(f32)
        routed = jnp.where(core == 0, block[:, own : own + 2], block[:, own + 2 :])
        r_s[h * 2 * nb : (h + 1) * 2 * nb] = routed.reshape(2 * nb, width).astype(bf16)
        x_s[h * half : (h + 1) * half] = block[:, :own].reshape(half, width).astype(bf16)
    rows = r_s[...]
    gate_pre = jnp.dot(rows, eg[0], preferred_element_type=f32)
    up_pre = jnp.dot(rows, eu[0], preferred_element_type=f32)
    act = clamped_unit(gate_pre, up_pre).astype(bf16)
    copies[0].wait()
    out = jnp.dot(act, d_s[...], preferred_element_type=f32).astype(bf16)
    some = slots // 2
    for r in range(2):
        to = lax.rem(core + r, 2) * nt
        for q in range(nt):
            msg[to + q, :, :wide] = out[r * some : (r + 1) * some, q * wide : (q + 1) * wide]
    x = x_s[...]
    gate = jnp.broadcast_to(bg[...].astype(f32), (8, width)).astype(bf16)
    branch = lax.dot_general(x, gate, (((1,), (1,)), ((), ())), preferred_element_type=f32)
    for copy in copies[1:]:
        copy.wait()
    pre = jnp.dot(x, w_s[...], preferred_element_type=f32)
    hidden = jax.nn.silu(pre[:, :cols]) * pre[:, cols:] * jax.nn.sigmoid(branch[:, 0:1])
    hidden = hidden.astype(bf16)
    for r in range(2):
        to = lax.rem(core + r, 2) * nt
        for q in range(nt):
            msg[to + q, :, wide : wide + cols] = hidden[r * half : r * half + some]
            msg[to + q, :, wide + cols :] = hidden[r * half + some : (r + 1) * half]


def block_kernel(at, got, dd, dd_other, him, lom, out, h_s):
    nt = got.shape[0] // 2
    some = got.shape[1]
    cols = dd.shape[0]
    wide = dd.shape[1]
    nb, seqs, _ = out.shape
    own = seqs // nt
    rows = []
    for c in range(2):
        part = jnp.sum(got[c * nt : (c + 1) * nt, :, :wide].astype(f32), axis=0)
        rows.append(part.astype(bf16))
        for q in range(nt):
            for f in range(2):
                start = wide + f * cols
                part = got[c * nt + q, :, start : start + cols].astype(f32)
                h_s[
                    f * nb // 2 : (f + 1) * nb // 2,
                    q * own : (q + 1) * own,
                    c * cols : (c + 1) * cols,
                ] = part.reshape(nb // 2, own, cols)
    hidden = h_s[...].reshape(nb * seqs, 2 * cols).astype(bf16)
    left = jnp.concatenate([hidden, him[...], lom[...]], axis=1)
    zero = at[2] == 0
    right = jnp.concatenate(
        [
            jnp.where(zero, dd[...], dd_other[...]),
            jnp.where(zero, dd_other[...], dd[...]),
            *rows,
            *rows,
        ],
        axis=0,
    )
    full = jnp.dot(left, right, preferred_element_type=f32)
    out[...] = full.astype(bf16).reshape(out.shape)


def final_kernel(got, res, out):
    out[...] = (jnp.sum(got[...].astype(f32), axis=0) + res[...]).astype(bf16)


def body(
    tokens,
    attn_gain,
    query_weight,
    key_weight,
    value_weight,
    break_bias,
    cache_keys,
    cache_values,
    lengths,
    out_weight,
    ffn_gain,
    branch_gate,
    dense_gate,
    dense_up,
    dense_down,
    route_ids,
    route_weights,
    expert_gate,
    expert_up,
    expert_down,
):
    nz, nt = lax.axis_size("z"), lax.axis_size("tp")
    nzx = nz * NX
    seqs, width = tokens.shape
    top = route_ids.shape[1]
    slice_width = width // nt
    all_rows = 2 * nzx * seqs
    slots = 2 * nzx * 2
    depth = query_weight.shape[0]
    heads = out_weight.shape[0]
    proj = query_weight.shape[1] + 2 * key_weight.shape[1]
    at = jnp.stack([lax.axis_index(a) for a in ("z", "x", "c", "tp")]).astype(jnp.int32)

    wcat, msg = local(
        functools.partial(prepare_kernel, nz),
        "prepare",
        [sds((depth, proj + 128)), sds((nz, depth, heads + 128))],
        (
            tokens,
            attn_gain[None],
            query_weight,
            key_weight,
            value_weight,
            out_weight.T,
            route_ids.T,
            route_weights.T,
        ),
        pin=pltpu.HBM,
    )
    with jax.named_scope("over_z"):
        got = exchange(msg, "z")
    with jax.named_scope("weights_x"):
        w_x = [wcat] + [along_x(wcat, k) for k in range(1, NX)]
    w_other = other_core(jnp.stack(w_x))
    part, owm = local(
        project_kernel,
        "project",
        [sds((nz, seqs, proj + 128)), sds((nz, depth, heads))],
        (at, got, *w_x, w_other),
        [pltpu.VMEM((2 * NX * depth, proj), bf16), pltpu.VMEM((nz * seqs, 2 * NX * depth), bf16)],
        smem=1,
    )
    with jax.named_scope("partial_z"):
        part = exchange(part, "z")
    with jax.named_scope("mix_x"):
        ow = [owm] + [along_x(owm, k) for k in range(1, NX)]
    ow_other = [other_core(piece) for piece in ow]

    attended, new_keys, new_values = attention(
        part, break_bias, cache_keys, cache_values, lengths
    )

    msg = local(
        mix_kernel,
        "mix",
        sds((nt, seqs, width)),
        (at, attended, *ow, *ow_other),
        [pltpu.VMEM((width, heads), bf16)],
        smem=1,
    )
    mixed = exchange(msg, "tp")
    him, lom = local(
        functools.partial(slots_kernel, seqs, top),
        "slots",
        [sds((all_rows // 2, slots))] * 2,
        (at, part),
        [pltpu.VMEM((all_rows // 2, 128), f32)],
        smem=1,
    )
    own = seqs // nt
    cols = dense_gate.shape[1]
    msg, resid = local(
        norm_kernel,
        "norm",
        [sds((nzx, 2 * own, width)), sds((seqs, slice_width), f32)],
        (at, mixed, tokens, ffn_gain[None], route_ids.T),
        smem=1,
    )
    with jax.named_scope("rows_zx"):
        mine = exchange(msg, ZX)
    with jax.named_scope("dense_tp"):
        gu = jnp.concatenate([dense_gate, dense_up], axis=1)
        gu = [gu] + [
            lax.ppermute(gu, "tp", [(i, (i + k) % nt) for i in range(nt)]) for k in range(1, nt)
        ]
        down = other_core(dense_down)
    mine, down, *gu = lax.optimization_barrier((mine, down, *gu))
    other, him, lom = lax.optimization_barrier((other_core(mine), him, lom))
    hbm = pl.BlockSpec(memory_space=pltpu.HBM)
    places = [pltpu.VMEM] * 2 + [pltpu.HBM] * nt + [pltpu.VMEM] * 3 + [pltpu.HBM]
    operands = (mine, other, *gu, branch_gate[None], expert_gate, expert_up, expert_down)
    msg = pl.pallas_call(
        expert_kernel,
        out_shape=pltpu.VMEM((2 * nt, slots // 2, slice_width + 2 * cols), bf16),
        in_specs=[SM] + [hbm if p == pltpu.HBM else VM for p in places],
        out_specs=VM,
        scratch_shapes=[
            pltpu.VMEM((width, 2 * cols), bf16),
            pltpu.VMEM(expert_down.shape[1:], bf16),
            pltpu.VMEM((2 * nzx * own, width), bf16),
            pltpu.VMEM((slots, width), bf16),
            pltpu.SemaphoreType.DMA((nt + 1,)),
        ],
        compiler_params=pltpu.CompilerParams(vmem_limit_bytes=16 << 20),
        name="expert",
    )(at, *(pltpu.with_memory_space_constraint(a, p) for a, p in zip(operands, places)))
    got = exchange(msg, ("c", "tp"))
    block = local(
        block_kernel,
        "block",
        sds((nzx, seqs, slice_width)),
        (at, got, dense_down, down, him, lom),
        [pltpu.VMEM((nzx, seqs, 2 * cols), f32)],
        smem=1,
    )
    got = exchange(block, ZX)
    out = local(final_kernel, "final", sds((seqs, slice_width)), (got, resid), keep=False)
    return out, new_keys, new_values


def solution(mesh):
    shape = (mesh.shape["ep"] // (2 * NX), NX, 2, mesh.shape["tp"])
    split = Mesh(mesh.devices.reshape(shape), ("z", "x", "c", "tp"))
    return jax.shard_map(
        body,
        mesh=split,
        in_specs=(
            P(EP, None),
            P(),
            P(EP, "tp"),
            P(EP, "tp"),
            P(EP, "tp"),
            P("tp"),
            P(EP, "tp", None, None),
            P(EP, "tp", None, None),
            P(EP),
            P("tp", EP),
            P(),
            P(),
            P("tp", EP),
            P("tp", EP),
            P(EP, "tp"),
            P(EP, None),
            P(EP, None),
            P(EP, None, "tp"),
            P(EP, None, "tp"),
            P(EP, "tp", None),
        ),
        out_specs=(P(EP, "tp"), P(EP, "tp"), P(EP, "tp")),
        check_vma=False,
    )
```
